32 devices in a mesh: kv: 16 (over z, y, x), tp: 2 (over core).
Axes of the slice: x: 2, y: 2, z: 4, core: 2. Of those that a mesh axis runs over, the one named last changes fastest.
Arguments:
- tokens: bfloat16 [64, 2048], P('tp', 'kv'), may hold values from -24 to 24
- lengths: int32 [16], P('kv'), may hold values from 1 to 4, 40 in all
- memory_state: float32 [16, 16, 128, 128], P('kv', 'tp'), may hold values from -3 to 3
- gain_first: float32 [2048], P('kv'), may hold values from 0.1 to 1.9
- first_gate: bfloat16 [2048, 5120], P('kv', 'tp'), may hold values from -0.125 to 0.125
- first_up: bfloat16 [2048, 5120], P('kv', 'tp'), may hold values from -0.125 to 0.125
- first_down: bfloat16 [5120, 2048], P('tp', 'kv'), may hold values from -0.15625 to 0.15625
- gain_mixer: float32 [2048], P('kv'), may hold values from 0.1 to 1.9
- query_weight: bfloat16 [2048, 2048], P('kv', 'tp'), may hold values from -0.125 to 0.125
- key_weight: bfloat16 [2048, 2048], P('kv', 'tp'), may hold values from -0.125 to 0.125
- value_weight: bfloat16 [2048, 2048], P('kv', 'tp'), may hold values from -0.125 to 0.125
- outgate_weight: bfloat16 [2048, 2048], P('kv', 'tp'), may hold values from -0.125 to 0.125
- beta_weight: bfloat16 [2048, 16], P('kv'), may hold values from -0.125 to 0.125
- decay_weight: bfloat16 [2048, 16], P('kv'), may hold values from -0.125 to 0.125
- decay_rate: float32 [16], P('tp'), may hold values from 0.05 to 4
- decay_bias: float32 [16], P('tp'), may hold values from -3 to 1
- head_gain: float32 [128], replicated, may hold values from 0.1 to 1.9
- out_weight: bfloat16 [2048, 2048], P('tp', 'kv'), may hold values from -0.25 to 0.25
- gain_second: float32 [2048], P('kv'), may hold values from 0.1 to 1.9
- second_gate: bfloat16 [2048, 5120], P('kv', 'tp'), may hold values from -0.125 to 0.125
- second_up: bfloat16 [2048, 5120], P('kv', 'tp'), may hold values from -0.125 to 0.125
- second_down: bfloat16 [5120, 2048], P('tp', 'kv'), may hold values from -0.15625 to 0.15625
Outputs:
- layer_out: bfloat16 [64, 2048], P('tp', 'kv')
- state_out: float32 [16, 16, 128, 128], P('kv', 'tp')
The draws below stay inside these ranges and needn't reach their ends.
Inputs may be any that keep to these rules, and one draw needn't show every extreme that they name: `lengths`: each sequence's count of live new token slots.
All inputs are finite; a program needn't handle non-finite values. No bound on the sum of `lengths` on one device may be relied on, other than what follows from the above.
Results may differ from the reference program's by a relative error of at most 0.02.
Values may be sent and summed in bfloat16 or wider, within the bound.
A program may use at most 64 MiB of HBM per device.

```python
import math
import jax
import jax.numpy as jnp
import numpy as np
from jax import lax

D = 2048
HEADS = 16
HEAD_DIM = 128
FF = 5120
NEW = 4
SEQS = 16
ROWS = 64


def draw_tokens(key, part):
    first_key = jax.random.fold_in(key, 0)
    column = jnp.arange(D, dtype=jnp.float32) / (D - 1)
    column_ramp = jnp.exp(jnp.log(0.5) + column * jnp.log(4.0))
    values = jax.random.normal(first_key, (ROWS, D), jnp.float32) * column_ramp
    return jnp.clip(values, -24.0, 24.0).astype(jnp.bfloat16)


def block_scale(rng, dims, cuts, smallest, high):
    def one(axis_at, parts):
        draws = jax.random.uniform(jax.random.fold_in(jax.random.fold_in(rng, 6), axis_at), (parts,), jnp.float32, smallest / len(cuts), high / len(cuts))
        return jnp.repeat(jnp.exp(draws), dims[axis_at] // parts).reshape((-1,) + (1,) * (len(dims) - axis_at - 1))

    loudness = one(*cuts[0])
    for cut in cuts[1:]:
        loudness = loudness * one(*cut)
    return loudness


def profile(number_of, total, most, slope):
    loads = [(1 << 20) // math.isqrt(grade ** slope) + 1 for grade in range(2, number_of + 1)]
    rest, given = total - most - (number_of - 1), [1] * (number_of - 1)
    while rest > 0:
        movable = [i for i in range(number_of - 1) if given[i] < most]
        pool, left = sum([loads[i] for i in movable]), rest
        for i in movable:
            addition = min(most - given[i], max(1, left * loads[i] // pool), rest)
            given[i] = given[i] + addition
            rest = rest - addition
    return np.array([most] + given)


def ragged(own_key, number_of, total, limit, slope):
    if number_of == 2:
        one = jax.random.randint(own_key, (), max(1, total - limit), min(limit, total - 1) + 1)
        return jnp.stack([one, total - one])
    sizes = jnp.asarray(profile(number_of, total, limit, slope), jnp.int32)
    pairs = (number_of - 1) // 2
    giver, receiver = sizes[1:1 + 2 * pairs:2], sizes[2:2 + 2 * pairs:2]
    margin = jnp.minimum(giver - 1, limit - receiver)
    moved = jax.random.randint(jax.random.fold_in(own_key, 1), (pairs,), 0, 1 << 20) % (margin + 1)
    sizes = sizes.at[1:1 + 2 * pairs:2].set(giver - moved).at[2:2 + 2 * pairs:2].set(receiver + moved)
    return sizes[jax.random.permutation(jax.random.fold_in(own_key, 2), number_of)]


def bell_draw(rng, shape, scale, reach, cuts=(), held_as=jnp.bfloat16):
    array = jax.random.normal(rng, shape, jnp.float32) * scale
    if len(cuts) > 0:
        array = block_scale(rng, shape, cuts, -0.22, 0.18) * array
    return jnp.clip(array, min=-reach, max=reach).astype(held_as)


def setup_inputs(seed: int = 0) -> dict:
    streams_of = jax.random.split(jax.random.key(seed), 23)
    tokens = draw_tokens(jax.random.fold_in(streams_of[22], 71), 0)
    lengths = ragged(streams_of[1], SEQS, (NEW + 1) * SEQS // 2, NEW, 2).astype(jnp.int32)
    memory_state = bell_draw(streams_of[2], (SEQS, HEADS, HEAD_DIM, HEAD_DIM), 0.5, 3.0, ((0, 16), (1, 2)), jnp.float32)
    gain_first = jnp.clip(1.0 + 0.18 * jax.random.normal(streams_of[3], (D,), jnp.float32), 0.1, 1.9)
    first_gate = bell_draw(streams_of[4], (D, FF), D ** -0.5, 0.125, ((0, 16), (1, 2)))
    first_up = bell_draw(streams_of[5], (D, FF), D ** -0.5, 0.125, ((0, 16), (1, 2)))
    first_down = bell_draw(streams_of[6], (FF, D), (FF // 4) ** -0.5, 0.15625, ((0, 2), (1, 16)))
    gain_mixer = jnp.clip(1.0 + 0.18 * jax.random.normal(streams_of[7], (D,), jnp.float32), 0.1, 1.9)
    query_weight = bell_draw(streams_of[8], (D, HEADS * HEAD_DIM), D ** -0.5, 0.125, ((0, 16), (1, 2)))
    key_weight = bell_draw(streams_of[9], (D, HEADS * HEAD_DIM), D ** -0.5, 0.125, ((0, 16), (1, 2)))
    value_weight = bell_draw(streams_of[10], (D, HEADS * HEAD_DIM), D ** -0.5, 0.125, ((0, 16), (1, 2)))
    outgate_weight = bell_draw(streams_of[11], (D, HEADS * HEAD_DIM), D ** -0.5, 0.125, ((0, 16), (1, 2)))
    beta_weight = bell_draw(streams_of[12], (D, HEADS), D ** -0.5, 0.125, ((0, 16),))
    decay_weight = bell_draw(streams_of[13], (D, HEADS), D ** -0.5, 0.125, ((0, 16),))
    decay_rate = jnp.clip(jnp.exp(math.log(4.0) - 4.3820266 * jax.random.uniform(streams_of[14], (HEADS,), jnp.float32) ** block_scale(streams_of[14], (HEADS,), ((0, 2),), -0.2, 0.2)), 0.05, 4.0)
    decay_bias = jnp.clip(-3.0 + 4.0 * jax.random.uniform(streams_of[15], (HEADS,), jnp.float32) ** block_scale(streams_of[15], (HEADS,), ((0, 2),), -0.2, 0.2), -3.0, 1.0)
    head_gain = jnp.clip(1.0 + 0.18 * jax.random.normal(streams_of[16], (HEAD_DIM,), jnp.float32), 0.1, 1.9)
    out_weight = bell_draw(streams_of[17], (HEADS * HEAD_DIM, D), (HEADS * HEAD_DIM // 4) ** -0.5, 0.25, ((0, 2), (1, 16)))
    gain_second = jnp.clip(1.0 + 0.18 * jax.random.normal(streams_of[18], (D,), jnp.float32), 0.1, 1.9)
    second_gate = bell_draw(streams_of[19], (D, FF), D ** -0.5, 0.125, ((0, 16), (1, 2)))
    second_up = bell_draw(streams_of[20], (D, FF), D ** -0.5, 0.125, ((0, 16), (1, 2)))
    second_down = bell_draw(streams_of[21], (FF, D), (FF // 4) ** -0.5, 0.15625, ((0, 2), (1, 16)))
    return {"tokens": tokens, "lengths": lengths, "memory_state": memory_state, "gain_first": gain_first, "first_gate": first_gate, "first_up": first_up, "first_down": first_down, "gain_mixer": gain_mixer, "query_weight": query_weight, "key_weight": key_weight, "value_weight": value_weight, "outgate_weight": outgate_weight, "beta_weight": beta_weight, "decay_weight": decay_weight, "decay_rate": decay_rate, "decay_bias": decay_bias, "head_gain": head_gain, "out_weight": out_weight, "gain_second": gain_second, "second_gate": second_gate, "second_up": second_up, "second_down": second_down}


EPS = 1e-06

def normed_operand(resid, gain):
    widened = resid.astype(jnp.float32)
    squares = lax.optimization_barrier(jnp.sum(widened * widened, axis=1))
    operand = (widened * gain).astype(jnp.bfloat16)
    return (operand, squares)

def inverse_rms(squares):
    return lax.rsqrt(squares / D + EPS)[:, None]

def advance(query_part, key_part, value_part, outgate_part, beta_logit, decay_logit, state_now, lengths, decay_rate, decay_bias, head_gain):
    seqs = state_now.shape[0]
    heads = state_now.shape[1]

    def split_heads(matrix):
        return matrix.reshape(seqs, NEW, heads, HEAD_DIM)
    query = split_heads(jax.nn.silu(query_part))
    query = query * lax.rsqrt(lax.optimization_barrier(jnp.sum(query * query, axis=-1, keepdims=True)) + EPS) * HEAD_DIM ** (-0.5)
    keyvec = split_heads(jax.nn.silu(key_part))
    keyvec = keyvec * lax.rsqrt(lax.optimization_barrier(jnp.sum(keyvec * keyvec, axis=-1, keepdims=True)) + EPS)
    values = split_heads(jax.nn.silu(value_part))
    live_mask = (jnp.arange(NEW, dtype=jnp.int32)[None, :] < lengths[:, None]).astype(jnp.float32)[:, :, None]
    beta_gate = jax.nn.sigmoid(beta_logit.reshape(seqs, NEW, heads)) * live_mask
    decay_log = -decay_rate * jax.nn.softplus(decay_logit.reshape(seqs, NEW, heads) + decay_bias) * live_mask
    outputs = []
    for position in range(NEW):
        state_now = state_now * jnp.exp(decay_log[:, position])[:, :, None, None]
        predicted = jnp.einsum('shk,shkv->shv', keyvec[:, position], state_now, precision=lax.Precision.HIGHEST)
        update = beta_gate[:, position][:, :, None] * (values[:, position] - predicted)
        state_now = state_now + keyvec[:, position][:, :, :, None] * update[:, :, None, :]
        outputs.append(jnp.einsum('shk,shkv->shv', query[:, position], state_now, precision=lax.Precision.HIGHEST))
    mixed = jnp.stack(outputs, axis=1) * live_mask[..., None]
    mixed = mixed * lax.rsqrt(lax.optimization_barrier(jnp.mean(mixed * mixed, axis=-1, keepdims=True)) + EPS) * head_gain
    mixed = mixed * jax.nn.silu(split_heads(outgate_part))
    return (mixed.reshape(seqs * NEW, heads * HEAD_DIM).astype(jnp.bfloat16), state_now)

def channel_mix(resid, gain, w_gate, w_up, w_down):
    operand, squares = normed_operand(resid, gain)
    scale = inverse_rms(squares)
    gate_part = jnp.dot(operand, w_gate, preferred_element_type=jnp.float32) * scale
    up_part = jnp.dot(operand, w_up, preferred_element_type=jnp.float32) * scale
    hidden = (jax.nn.silu(gate_part) * up_part).astype(jnp.bfloat16)
    branch = jnp.dot(hidden, w_down, preferred_element_type=jnp.float32)
    return (resid.astype(jnp.float32) + 0.5 * branch).astype(jnp.bfloat16)

def reference(tokens, lengths, memory_state, gain_first, first_gate, first_up, first_down, gain_mixer, query_weight, key_weight, value_weight, outgate_weight, beta_weight, decay_weight, decay_rate, decay_bias, head_gain, out_weight, gain_second, second_gate, second_up, second_down):
    first = channel_mix(tokens, gain_first, first_gate, first_up, first_down)
    operand, squares = normed_operand(first, gain_mixer)
    scale = inverse_rms(squares)

    def project(weight):
        return jnp.dot(operand, weight, preferred_element_type=jnp.float32) * scale
    mixed, state_out = advance(project(query_weight), project(key_weight), project(value_weight), project(outgate_weight), project(beta_weight), project(decay_weight), memory_state, lengths, decay_rate, decay_bias, head_gain)
    second = (first.astype(jnp.float32) + jnp.dot(mixed, out_weight, preferred_element_type=jnp.float32)).astype(jnp.bfloat16)
    layer_out = channel_mix(second, gain_second, second_gate, second_up, second_down)
    return (layer_out, state_out)
```

```python
import functools

import jax
import jax.numpy as jnp
from jax import lax
from jax.experimental import pallas as pl
from jax.experimental.pallas import tpu as pltpu
from jax.sharding import PartitionSpec as P

MESH = pl.DeviceIdType.MESH
HEAD_DIM = 128
LANES = 128
NEW = 4
EPS = 1e-06
F32 = jnp.float32
BF16 = jnp.bfloat16


def silu(x):
    return x / (1.0 + jnp.exp(-x))


def pieces(total, most):
    return next(k for k in range(most, 0, -1) if total % k == 0)


def swaps(count):
    return count > 2


def early_of(count):
    return min(1, count - 1 - int(swaps(count)))


def chunks_of(total, step):
    return [(c, min(step, total - c)) for c in range(0, total, step)]


def layer_kernel(
    n,
    tps,
    tokens,
    lengths,
    state_hbm,
    gain_first,
    first_gate_hbm,
    first_up_hbm,
    first_down_hbm,
    gain_mixer,
    query_hbm,
    key_hbm,
    value_hbm,
    outgate_hbm,
    beta_weight,
    decay_weight,
    decay_rate,
    decay_bias,
    head_gain,
    out_hbm,
    gain_second,
    second_gate_hbm,
    second_up_hbm,
    second_down_hbm,
    layer_out,
    state_out_hbm,
    first_gate,
    first_up,
    first_down,
    query_w,
    key_w,
    value_w,
    outgate_w,
    out_w,
    second_gate,
    second_up,
    second_down,
    state,
    new_state,
    resid,
    spread_top,
    spread_low,
    arrived,
    natural,
    first_sums,
    mixer_sums,
    second_sums,
    hidden_first,
    hidden_mixer,
    hidden_second,
    pair_first,
    pair_mixer,
    pair_second,
    load_sem,
    send_sem,
    recv_sem,
    pair_sem,
    early_sem,
    turn_sem,
):
    me = lax.axis_index("kv")
    my_tp = lax.axis_index("tp")
    rows, width = resid.shape
    own_rows = rows // tps
    group = hidden_first.shape[0]
    depth = n // group
    my_plane, my_depth = lax.rem(me, group), me // group
    heads = state.shape[0]
    model = n * width
    paired = tps % 2 == 0
    late = lax.rem(my_tp, 2) == 1
    partner = my_tp + 1 - 2 * lax.rem(my_tp, 2)

    barrier = pltpu.get_barrier_semaphore()

    def greet_plane(step, carry):
        to = my_depth * group + lax.rem(my_plane + step, group)
        pl.semaphore_signal(barrier, inc=1, device_id={"kv": to}, device_id_type=MESH)
        return carry

    def greet_depth(step, carry):
        to = lax.rem(my_depth + step, depth) * group + my_plane
        pl.semaphore_signal(barrier, inc=1, device_id={"kv": to}, device_id_type=MESH)
        return carry

    def greet_tp(step, carry):
        pl.semaphore_signal(
            barrier, inc=1, device_id={"tp": lax.rem(my_tp + step, tps)}, device_id_type=MESH
        )
        return carry

    lax.fori_loop(1, depth, greet_depth, 0)
    lax.fori_loop(1, group, greet_plane, 0)
    lax.fori_loop(1, tps, greet_tp, 0)

    loads = []
    for at, (src, dst) in enumerate(
        (
            (first_gate_hbm, first_gate),
            (first_up_hbm, first_up),
            (first_down_hbm, first_down),
            (query_hbm, query_w),
            (key_hbm, key_w),
            (value_hbm, value_w),
            (outgate_hbm, outgate_w),
            (state_hbm.at[0], state),
            (out_hbm, out_w),
            (second_gate_hbm, second_gate),
            (second_up_hbm, second_up),
            (second_down_hbm, second_down),
        )
    ):
        load = pltpu.make_async_copy(src, dst, load_sem.at[at])
        load.start()
        loads.append(load)

    spread_rows, half = 2 * rows, NEW
    at_row = lax.broadcasted_iota(jnp.int32, (spread_rows, rows), 0)
    at_col = lax.broadcasted_iota(jnp.int32, (spread_rows, rows), 1)
    source = (at_row // (2 * half)) * half + at_row % half
    top = (at_row % (2 * half)) < half
    hit = source == at_col
    spread_top[...] = jnp.where(hit & top, 1.0, 0.0).astype(BF16)
    spread_low[...] = jnp.where(hit & jnp.logical_not(top), 1.0, 0.0).astype(BF16)

    own = pl.ds(pl.multiple_of(my_tp * own_rows, own_rows), own_rows)
    arrived[own, :] = tokens[...].astype(F32)
    place_row = lax.broadcasted_iota(jnp.int32, (rows, rows), 0)
    place_col = lax.broadcasted_iota(jnp.int32, (rows, rows), 1)
    block = place_row // half
    wanted = ((block % depth) * group + block // depth) * half + place_row % half
    natural[...] = jnp.where(wanted == place_col, 1.0, 0.0).astype(BF16)
    pl.semaphore_wait(barrier, depth - 1 + group - 1 + tps - 1)

    def all_tp(src, dst, stage, part):
        def one(step, carry):
            pltpu.make_async_remote_copy(
                src_ref=src,
                dst_ref=dst,
                send_sem=pair_sem.at[0, stage],
                recv_sem=pair_sem.at[1, stage],
                device_id={"tp": lax.rem(my_tp + step, tps)},
                device_id_type=MESH,
            ).start()
            return carry

        lax.fori_loop(1, tps, one, 0)

        def settle(sem):
            def one_wait(step, carry):
                pltpu.make_async_copy(part, part, sem).wait()
                return carry

            lax.fori_loop(1, tps, one_wait, 0)

        settle(pair_sem.at[1, stage])
        settle(pair_sem.at[0, stage])

    all_tp(arrived.at[own, :], arrived.at[own, :], 0, arrived.at[pl.ds(0, own_rows), :])
    resid[...] = jnp.dot(
        natural[...], arrived[...].astype(BF16), preferred_element_type=F32
    )

    def spread(matrix_top, matrix_low):
        low = jnp.dot(spread_low[...], matrix_low, preferred_element_type=F32)
        high = jnp.dot(spread_top[...], matrix_top, preferred_element_type=F32)
        return high, low

    def norm_operand(gain):
        whole = resid[...]
        squares = jnp.sum(whole * whole, axis=1, keepdims=True)
        operand = (whole * gain[...]).astype(BF16)
        squares_top = squares.astype(BF16)
        squares_low = (squares - squares_top.astype(F32)).astype(BF16)
        high, low = spread(operand, operand)
        sq_high, sq_low = spread(
            jnp.broadcast_to(squares_top.astype(F32), (rows, LANES)).astype(BF16),
            jnp.broadcast_to(squares_low.astype(F32), (rows, LANES)).astype(BF16),
        )
        return high.astype(BF16), low.astype(BF16), sq_high + sq_low

    def rs_first(bufs, sems, c, start, size, swapped):
        send, mid, _, _, swap_mid, _, _, _, _, _ = bufs
        cols = pl.ds(start, size)
        stage = sems // 6
        if paired and not swapped and c == 0:

            @pl.when(late)
            def _():
                pl.semaphore_wait(turn_sem.at[stage], 1)

        if swapped:
            count, place, sem = depth, my_depth, sems + 4
        else:
            count, place, sem = group, my_plane, sems

        def source(to):
            return send.at[:, to, :, cols] if swapped else send.at[to, :, :, cols]

        early = not swapped and c == early_of(bufs[8])
        target = swap_mid.at[place] if swapped else mid.at[place, :, :, cols]
        pltpu.make_async_copy(source(place), target, recv_sem.at[sems, c]).start()

        def one(step, carry):
            to = lax.rem(place + step, count)
            kv = to * group + my_plane if swapped else my_depth * group + to
            pltpu.make_async_remote_copy(
                src_ref=source(to),
                dst_ref=target,
                send_sem=early_sem.at[stage] if early else send_sem.at[sem],
                recv_sem=recv_sem.at[sems, c],
                device_id={"kv": kv},
                device_id_type=MESH,
            ).start()
            return carry

        lax.fori_loop(1, count, one, 0)

    def early_part(bufs, start, size):
        return bufs[1].at[pl.ds(0, group - 1), :, :, pl.ds(start, size)]

    def hand_over(bufs, sems, start, size):
        part = early_part(bufs, start, size)
        pltpu.make_async_copy(part, part, early_sem.at[sems // 6]).wait()
        if paired:

            @pl.when(jnp.logical_not(late))
            def _():
                pl.semaphore_signal(
                    turn_sem.at[sems // 6], inc=1, device_id={"tp": partner}, device_id_type=MESH
                )

    def rs_second(bufs, sems, c, start, size, swapped):
        _, mid, red, fin, swap_mid, swap_red, swap_fin, _, _, _ = bufs
        if swapped:
            came, kept, last, base = swap_mid, swap_red, swap_fin, 0
            count, place, sem = group, my_plane, sems + 5
        else:
            came, kept, last, base = mid, red, fin, start
            count, place, sem = depth, my_depth, sems + 1
        cols = pl.ds(base, size)
        part = came.at[:, :, :, cols]
        pltpu.make_async_copy(part, part, recv_sem.at[sems, c]).wait()
        for d in range(count):
            for at, wide in chunks_of(size, 512):
                span_at = slice(base + at, base + at + wide)
                value = came[0, d, :, span_at].astype(F32)
                for g in range(1, came.shape[0]):
                    value = value + came[g, d, :, span_at].astype(F32)
                kept[d, :, span_at] = value.astype(BF16)
        pltpu.make_async_copy(
            kept.at[place, :, cols], last.at[place, :, cols], recv_sem.at[sems + 1, c]
        ).start()

        def one(step, carry):
            to = lax.rem(place + step, count)
            kv = my_depth * group + to if swapped else to * group + my_plane
            pltpu.make_async_remote_copy(
                src_ref=kept.at[to, :, cols],
                dst_ref=last.at[place, :, cols],
                send_sem=send_sem.at[sem],
                recv_sem=recv_sem.at[sems + 1, c],
                device_id={"kv": kv},
                device_id_type=MESH,
            ).start()
            return carry

        lax.fori_loop(1, count, one, 0)

    def rs_wait(bufs, sems, c, start, size, swapped):
        part = bufs[6] if swapped else bufs[3].at[:, :, pl.ds(start, size)]
        pltpu.make_async_copy(part, part, recv_sem.at[sems + 1, c]).wait()

    def ag_depth(bufs, sems, c, start, size):
        buffer = bufs[7]
        mine = buffer.at[my_plane, my_depth, :, pl.ds(start, size)]

        def one(step, carry):
            pltpu.make_async_remote_copy(
                src_ref=mine,
                dst_ref=mine,
                send_sem=send_sem.at[sems + 2],
                recv_sem=recv_sem.at[sems + 2, c],
                device_id={"kv": lax.rem(my_depth + step, depth) * group + my_plane},
                device_id_type=MESH,
            ).start()
            return carry

        lax.fori_loop(1, depth, one, 0)

    def ag_plane(bufs, sems, c, start, size):
        buffer = bufs[7]
        cols = pl.ds(start, size)
        part = buffer.at[0, pl.ds(0, depth - 1), :, cols]
        pltpu.make_async_copy(part, part, recv_sem.at[sems + 2, c]).wait()
        mine = buffer.at[my_plane, :, :, cols]

        def one(step, carry):
            pltpu.make_async_remote_copy(
                src_ref=mine,
                dst_ref=mine,
                send_sem=send_sem.at[sems + 3],
                recv_sem=recv_sem.at[sems + 3, c],
                device_id={"kv": my_depth * group + lax.rem(my_plane + step, group)},
                device_id_type=MESH,
            ).start()
            return carry

        lax.fori_loop(1, group, one, 0)

    def ag_wait(bufs, sems, c, start, size):
        part = bufs[7].at[pl.ds(0, group - 1), :, :, pl.ds(start, size)]
        pltpu.make_async_copy(part, part, recv_sem.at[sems + 3, c]).wait()

    def all_sent(bufs, sems):
        send, mid, red, fin, swap_mid, swap_red, swap_fin, buffer, _, width = bufs
        parts = [
            mid.at[pl.ds(0, group - 1), :, :, pl.ds(0, mid.shape[3] - width)],
            fin.at[pl.ds(0, depth - 1)],
            buffer.at[0, pl.ds(0, depth - 1)],
            buffer.at[pl.ds(0, group - 1)],
        ]
        if mid.shape[3] < send.shape[3]:
            parts += [swap_mid.at[pl.ds(0, depth - 1)], swap_fin.at[pl.ds(0, group - 1)]]
        for at, part in enumerate(parts):
            if min(part.shape) > 0:
                pltpu.make_async_copy(part, part, send_sem.at[sems + at]).wait()

    def put(send, start, size, value):
        send[:, :, :, start : start + size] = value.reshape(group, depth, 2 * half, size).astype(
            BF16
        )

    def total(bufs, start, size):
        fin, begin = bufs[3], start
        if start >= fin.shape[2]:
            fin, begin = bufs[6], start - fin.shape[2]
        value = fin[0, :, begin : begin + size].astype(F32)
        for k in range(1, fin.shape[0]):
            value = value + fin[k, :, begin : begin + size].astype(F32)
        return value

    def inverse_rms(bufs):
        squares = total(bufs, 0, LANES)
        return lax.rsqrt((squares[:half] + squares[half:]) / model + EPS)

    def stacked(buffer, start, size):
        flat = buffer[:, :, :, start : start + size].astype(F32).reshape(rows, size)
        return flat.astype(BF16)

    def in_order(count):
        order = list(range(count))
        if swaps(count):
            order = order[: count - 2] + [count - 1, count - 2]
        return [(stage, c) for stage in range(4) for c in order]

    def in_issue(count):
        order = list(range(count))
        return order[-1:] + order[:-1] if swaps(count) else order

    def feed_forward(gain, gate, up, down, waits, bufs, pair, sems, tp_sems):
        send, hidden = bufs[0], bufs[7]
        high, low, squares = norm_operand(gain)
        units = gate.shape[1]
        count = pieces(units // LANES, 4)
        size = units // count
        put(send, 0, LANES, squares)
        waits[0].wait()
        waits[1].wait()

        def sums_at(c):
            swapped = swaps(count) and c == count - 1
            return (0, LANES + size, False) if c == 0 else (LANES + c * size, size, swapped)

        for c in in_issue(count):
            for at, wide in chunks_of(size, 512):
                lo = c * size + at
                put(
                    send,
                    LANES + lo,
                    wide,
                    jnp.dot(high, gate[:, lo : lo + wide], preferred_element_type=F32)
                    + jnp.dot(low, up[:, lo : lo + wide], preferred_element_type=F32),
                )
            rs_first(bufs, sems, c, *sums_at(c))
        hand_over(bufs, sems, *sums_at(early_of(count))[:2])
        branch = jnp.zeros((rows, width), F32)
        scale, down_ready = None, []
        for stage, c in in_order(count):
            if stage == 0:
                rs_second(bufs, sems, c, *sums_at(c))
            elif stage == 1:
                rs_wait(bufs, sems, c, *sums_at(c))
                if c == 0:
                    scale = inverse_rms(bufs)
                for at, wide in chunks_of(size, LANES):
                    lo = c * size + at
                    both = total(bufs, LANES + lo, wide)
                    hidden[my_plane, my_depth, :, lo : lo + wide] = (
                        silu(both[:half] * scale) * (both[half:] * scale)
                    ).astype(BF16)
                ag_depth(bufs, sems, c, c * size, size)
            elif stage == 2:
                ag_plane(bufs, sems, c, c * size, size)
            else:
                ag_wait(bufs, sems, c, c * size, size)
                if not down_ready:
                    down_ready.append(waits[2].wait())
                branch = branch + jnp.dot(
                    stacked(hidden, c * size, size),
                    down[c * size : (c + 1) * size, :],
                    preferred_element_type=F32,
                )
        pair[my_tp] = branch
        all_tp(pair.at[my_tp], pair.at[my_tp], tp_sems, pair.at[0])
        branch = pair[0]
        for t in range(1, tps):
            branch = branch + pair[t]
        resid[...] = (resid[...] + 0.5 * branch).astype(BF16).astype(F32)

    half_count = pieces(first_gate.shape[1] // LANES, 4)
    half_size = first_gate.shape[1] // half_count
    mixer_count = pieces(heads, 4)
    mixer_size = 2 * heads * HEAD_DIM // mixer_count

    def early_width(before, parts, each):
        return each if early_of(parts) else before + each

    half_early = (half_count, early_width(LANES, half_count, half_size))
    mixer_early = (mixer_count, early_width(2 * LANES, mixer_count, mixer_size))
    first_bufs = (*first_sums, hidden_first, *half_early)
    mixer_bufs = (*mixer_sums, hidden_mixer, *mixer_early)
    second_bufs = (*second_sums, hidden_second, *half_early)
    send_mixer = mixer_sums[0]
    feed_forward(
        gain_first, first_gate, first_up, first_down, loads[0:3],
        first_bufs, pair_first, 0, 1,
    )

    high, low, squares = norm_operand(gain_mixer)
    all_heads = beta_weight.shape[0]
    across = (((1,), (1,)), ((), ()))
    put(send_mixer, 0, LANES, squares)
    send_mixer[:, :, :, LANES : 2 * LANES] = jnp.zeros((group, depth, 2 * half, LANES), BF16)
    small = lax.dot_general(
        high, beta_weight[...], across, preferred_element_type=F32
    ) + lax.dot_general(low, decay_weight[...], across, preferred_element_type=F32)
    put(send_mixer, LANES, all_heads, small)
    for load in loads[3:7]:
        load.wait()
    count = pieces(heads, 4)
    batch = heads // count
    size = batch * HEAD_DIM

    def mixed_at(c):
        start = 2 * LANES + 2 * c * size
        swapped = swaps(count) and c == count - 1
        return (0, 2 * LANES + 2 * size, False) if c == 0 else (start, 2 * size, swapped)

    for c in in_issue(count):
        for at, (first, second) in enumerate(((query_w, value_w), (key_w, outgate_w))):
            lo = c * size
            put(
                send_mixer,
                2 * LANES + (2 * c + at) * size,
                size,
                jnp.dot(high, first[:, lo : lo + size], preferred_element_type=F32)
                + jnp.dot(low, second[:, lo : lo + size], preferred_element_type=F32),
            )
        rs_first(mixer_bufs, 6, c, *mixed_at(c))
    hand_over(mixer_bufs, 6, *mixed_at(early_of(count))[:2])
    lane = lax.broadcasted_iota(jnp.int32, (half, LANES), 1)
    slot = lax.broadcasted_iota(jnp.int32, (half, LANES), 0)
    live = jnp.where(slot < lengths[0], 1.0, 0.0)
    scale, logits = None, None
    branch = jnp.zeros((rows, width), F32)
    for stage, c in in_order(count):
        if stage == 0:
            rs_second(mixer_bufs, 6, c, *mixed_at(c))
            continue
        if stage == 2:
            ag_plane(mixer_bufs, 6, c, c * size, size)
            continue
        if stage == 3:
            ag_wait(mixer_bufs, 6, c, c * size, size)
            if c == 0:
                loads[8].wait()
            branch = branch + jnp.dot(
                stacked(hidden_mixer, c * size, size),
                out_w[c * size : (c + 1) * size, :],
                preferred_element_type=F32,
            )
            continue
        rs_wait(mixer_bufs, 6, c, *mixed_at(c))
        if c == 0:
            scale = inverse_rms(mixer_bufs)
            logits = total(mixer_bufs, LANES, LANES)
            loads[7].wait()
        for h in range(c * batch, (c + 1) * batch):
            base = 2 * LANES + 2 * c * size + (h - c * batch) * HEAD_DIM
            both = total(mixer_bufs, base, HEAD_DIM)
            query, value = silu(both[:half] * scale), silu(both[half:] * scale)
            both = total(mixer_bufs, base + size, HEAD_DIM)
            keyvec, outgate = silu(both[:half] * scale), silu(both[half:] * scale)
            query = query * lax.rsqrt(jnp.sum(query * query, axis=1, keepdims=True) + EPS)
            query = query * HEAD_DIM ** (-0.5)
            keyvec = keyvec * lax.rsqrt(jnp.sum(keyvec * keyvec, axis=1, keepdims=True) + EPS)
            mine = lane == my_tp * heads + h
            beta_logit = jnp.sum(jnp.where(mine, logits[:half] * scale, 0.0), axis=1, keepdims=True)
            decay_logit = jnp.sum(jnp.where(mine, logits[half:] * scale, 0.0), axis=1, keepdims=True)
            beta_logit = jnp.broadcast_to(beta_logit, (half, LANES))
            decay_logit = jnp.broadcast_to(decay_logit, (half, LANES)) + decay_bias[0, h]
            beta = live / (1.0 + jnp.exp(-beta_logit))
            soft = jnp.maximum(decay_logit, 0.0) + jnp.log(1.0 + jnp.exp(-jnp.abs(decay_logit)))
            decay = -decay_rate[0, h] * soft * live
            reach = jnp.zeros_like(decay)
            for i in range(NEW):
                reach = reach + jnp.where(slot >= i, decay[i : i + 1], 0.0)
            before = jnp.exp(reach)
            old = state[h]
            held = jnp.dot(
                jnp.concatenate([keyvec, query], axis=0),
                old,
                precision=lax.Precision.HIGHEST,
                preferred_element_type=F32,
            )
            update = beta * (value - before * held[:half])
            output = before * held[half:]
            for i in range(NEW):
                between = jnp.where(slot >= i, jnp.exp(jnp.minimum(reach - reach[i : i + 1], 0.0)), 0.0)
                row = keyvec[i : i + 1]
                alike = jnp.sum(keyvec * row, axis=1, keepdims=True)
                fixed = update[i : i + 1]
                update = update - jnp.where(slot > i, beta * between * alike * fixed, 0.0)
                output = output + between * jnp.sum(query * row, axis=1, keepdims=True) * fixed
            last = reach[NEW - 1 : NEW]
            gained = update * jnp.exp(last - reach)
            zero = jnp.zeros_like(keyvec)
            new_state[h] = old * jnp.exp(last) + lax.dot_general(
                jnp.concatenate([keyvec, zero], axis=0),
                jnp.concatenate([gained, zero], axis=0),
                (((0,), (0,)), ((), ())),
                precision=lax.Precision.HIGHEST,
                preferred_element_type=F32,
            )
            output = output * live
            output = output * lax.rsqrt(jnp.mean(output * output, axis=1, keepdims=True) + EPS)
            output = output * head_gain[...] * outgate
            hidden_mixer[my_plane, my_depth, :, h * HEAD_DIM : (h + 1) * HEAD_DIM] = output.astype(
                BF16
            )
        ag_depth(mixer_bufs, 6, c, c * size, size)
    save = pltpu.make_async_copy(new_state, state_out_hbm.at[0], load_sem.at[12])
    save.start()
    pair_mixer[my_tp] = branch
    all_tp(pair_mixer.at[my_tp], pair_mixer.at[my_tp], 2, pair_mixer.at[0])
    branch = pair_mixer[0]
    for t in range(1, tps):
        branch = branch + pair_mixer[t]
    resid[...] = (resid[...] + branch).astype(BF16).astype(F32)

    feed_forward(
        gain_second, second_gate, second_up, second_down, loads[9:12],
        second_bufs, pair_second, 12, 3,
    )
    arrived[...] = lax.dot_general(
        natural[...], resid[...].astype(BF16), (((0,), (0,)), ((), ())), preferred_element_type=F32
    )
    layer_out[...] = arrived[own, :].astype(BF16)
    save.wait()
    all_sent(first_bufs, 0)
    all_sent(mixer_bufs, 6)
    all_sent(second_bufs, 12)


def solution(mesh):
    n, tps = mesh.shape["kv"], mesh.shape["tp"]

    def on_device(
        tokens,
        lengths,
        memory_state,
        gain_first,
        first_gate,
        first_up,
        first_down,
        gain_mixer,
        query_weight,
        key_weight,
        value_weight,
        outgate_weight,
        beta_weight,
        decay_weight,
        decay_rate,
        decay_bias,
        head_gain,
        out_weight,
        gain_second,
        second_gate,
        second_up,
        second_down,
    ):
        rows = tokens.shape[0] * tps
        width = tokens.shape[1]
        units = first_gate.shape[1]
        span = query_weight.shape[1]
        group = pieces(n, 4)
        depth = n // group
        half_parts = pieces(units // LANES, 4)
        mixer_parts = pieces(memory_state.shape[1], 4)
        vmem = pl.BlockSpec(memory_space=pltpu.VMEM)
        smem = pl.BlockSpec(memory_space=pltpu.SMEM)
        hbm = pl.BlockSpec(memory_space=pl.ANY)

        def like(array):
            return pltpu.VMEM(array.shape, array.dtype)

        def owners(before, parts, each):
            last = each if swaps(parts) else LANES
            columns = before + parts * each
            kept = columns - (last if swaps(parts) else 0)
            return (
                pltpu.VMEM((group, depth, 2 * NEW, columns), BF16),
                pltpu.VMEM((group, depth, 2 * NEW, kept), BF16),
                pltpu.VMEM((depth, 2 * NEW, kept), BF16),
                pltpu.VMEM((depth, 2 * NEW, kept), BF16),
                pltpu.VMEM((depth, group, 2 * NEW, last), BF16),
                pltpu.VMEM((group, 2 * NEW, last), BF16),
                pltpu.VMEM((group, 2 * NEW, last), BF16),
            )

        def gathered(columns):
            return pltpu.VMEM((group, depth, NEW, columns), BF16)

        def pairs():
            return pltpu.VMEM((tps, rows, width), F32)

        return pl.pallas_call(
            functools.partial(layer_kernel, n, tps),
            name="layer",
            out_shape=(
                jax.ShapeDtypeStruct(tokens.shape, BF16),
                jax.ShapeDtypeStruct(memory_state.shape, F32),
            ),
            in_specs=[
                vmem, smem, hbm, vmem, hbm, hbm, hbm, vmem, hbm, hbm, hbm, hbm,
                vmem, vmem, smem, smem, vmem, hbm, vmem, hbm, hbm, hbm,
            ],
            out_specs=(vmem, hbm),
            scratch_shapes=[
                like(first_gate),
                like(first_up),
                like(first_down),
                like(query_weight),
                like(key_weight),
                like(value_weight),
                like(outgate_weight),
                like(out_weight),
                like(second_gate),
                like(second_up),
                like(second_down),
                pltpu.VMEM(memory_state.shape[1:], F32),
                pltpu.VMEM(memory_state.shape[1:], F32),
                pltpu.VMEM((rows, width), F32),
                pltpu.VMEM((2 * rows, rows), BF16),
                pltpu.VMEM((2 * rows, rows), BF16),
                pltpu.VMEM((rows, width), F32),
                pltpu.VMEM((rows, rows), BF16),
                owners(LANES, half_parts, units // half_parts),
                owners(2 * LANES, mixer_parts, 2 * span // mixer_parts),
                owners(LANES, half_parts, units // half_parts),
                gathered(units),
                gathered(span),
                gathered(units),
                pairs(),
                pairs(),
                pairs(),
                pltpu.SemaphoreType.DMA((13,)),
                pltpu.SemaphoreType.DMA((18,)),
                pltpu.SemaphoreType.DMA((18, 4)),
                pltpu.SemaphoreType.DMA((2, 4)),
                pltpu.SemaphoreType.DMA((3,)),
                pltpu.SemaphoreType.REGULAR((3,)),
            ],
            compiler_params=pltpu.CompilerParams(
                collective_id=0,
                has_side_effects=True,
                vmem_limit_bytes=60 * 1024 * 1024,
            ),
        )(
            tokens,
            lengths,
            memory_state,
            gain_first.reshape(1, -1),
            first_gate,
            first_up,
            first_down,
            gain_mixer.reshape(1, -1),
            query_weight,
            key_weight,
            value_weight,
            outgate_weight,
            beta_weight.T,
            decay_weight.T,
            decay_rate.reshape(1, -1),
            decay_bias.reshape(1, -1),
            head_gain.reshape(1, -1),
            out_weight,
            gain_second.reshape(1, -1),
            second_gate,
            second_up,
            second_down,
        )

    in_specs = (
        P("tp", "kv"),
        P("kv"),
        P("kv", "tp", None, None),
        P("kv"),
        P("kv", "tp"),
        P("kv", "tp"),
        P("tp", "kv"),
        P("kv"),
        P("kv", "tp"),
        P("kv", "tp"),
        P("kv", "tp"),
        P("kv", "tp"),
        P("kv", None),
        P("kv", None),
        P("tp"),
        P("tp"),
        P(),
        P("tp", "kv"),
        P("kv"),
        P("kv", "tp"),
        P("kv", "tp"),
        P("tp", "kv"),
    )
    out_specs = (P("tp", "kv"), P("kv", "tp", None, None))
    return jax.shard_map(
        on_device, mesh=mesh, in_specs=in_specs, out_specs=out_specs, check_vma=False
    )
```

```python
import functools

import jax
import jax.numpy as jnp
from jax import lax
from jax.experimental import pallas as pl
from jax.experimental.pallas import tpu as pltpu
from jax.sharding import PartitionSpec as P

MESH = pl.DeviceIdType.MESH
HEAD_DIM = 128
LANES = 128
NEW = 4
EPS = 1e-06
EARLY = 1
HALF_DIRECT = 2
MIXER_DIRECT = 4
F32 = jnp.float32
BF16 = jnp.bfloat16


def silu(x):
    return x / (1.0 + jnp.exp(-x))


def pieces(total, most):
    return next(k for k in range(most, 0, -1) if total % k == 0)


def swaps(count):
    return count > 2


def early_of(count):
    return min(EARLY, count - 1 - int(swaps(count)))


def chunks_of(total, step):
    return [(c, min(step, total - c)) for c in range(0, total, step)]


def put_out(layer, state, layer_hbm, state_hbm, sem):
    moves = [
        pltpu.make_async_copy(src, dst, sem.at[at])
        for at, (src, dst) in enumerate(((layer, layer_hbm), (state, state_hbm)))
    ]
    for move in moves:
        move.start()
    for move in moves:
        move.wait()


def layer_kernel(
    n,
    tps,
    tokens_hbm,
    lengths_hbm,
    state_hbm,
    gain_first_hbm,
    first_gate_hbm,
    first_up_hbm,
    first_down_hbm,
    gain_mixer_hbm,
    query_hbm,
    key_hbm,
    value_hbm,
    outgate_hbm,
    beta_hbm,
    decay_hbm,
    rate_hbm,
    bias_hbm,
    head_gain_hbm,
    out_hbm,
    gain_second_hbm,
    second_gate_hbm,
    second_up_hbm,
    second_down_hbm,
    layer_out,
    new_state,
    tokens,
    lengths,
    gain_first,
    gain_mixer,
    beta_weight,
    decay_weight,
    decay_rate,
    decay_bias,
    head_gain,
    gain_second,
    first_gate,
    first_up,
    first_down,
    query_w,
    key_w,
    value_w,
    outgate_w,
    out_w,
    second_gate,
    second_up,
    second_down,
    state,
    resid,
    spread_top,
    spread_low,
    arrived,
    natural,
    first_sums,
    mixer_sums,
    second_sums,
    hidden_first,
    hidden_mixer,
    hidden_second,
    pair_first,
    pair_mixer,
    pair_second,
    load_sem,
    send_sem,
    recv_sem,
    pair_sem,
    early_sem,
    turn_sem,
    small_sem,
):
    me = lax.axis_index("kv")
    my_tp = lax.axis_index("tp")
    rows, width = resid.shape
    own_rows = rows // tps
    group = hidden_first.shape[0]
    depth = n // group
    my_plane, my_depth = lax.rem(me, group), me // group
    heads = state.shape[0]
    model = n * width
    paired = tps % 2 == 0
    late = lax.rem(my_tp, 2) == 1
    partner = my_tp + 1 - 2 * lax.rem(my_tp, 2)

    barrier = pltpu.get_barrier_semaphore()

    def greet_plane(step, carry):
        to = my_depth * group + lax.rem(my_plane + step, group)
        pl.semaphore_signal(barrier, inc=1, device_id={"kv": to}, device_id_type=MESH)
        return carry

    def greet_depth(step, carry):
        to = lax.rem(my_depth + step, depth) * group + my_plane
        pl.semaphore_signal(barrier, inc=1, device_id={"kv": to}, device_id_type=MESH)
        return carry

    def greet_tp(step, carry):
        pl.semaphore_signal(
            barrier, inc=1, device_id={"tp": lax.rem(my_tp + step, tps)}, device_id_type=MESH
        )
        return carry

    lax.fori_loop(1, depth, greet_depth, 0)
    lax.fori_loop(1, group, greet_plane, 0)
    lax.fori_loop(1, tps, greet_tp, 0)

    smalls = []
    for at, (src, dst) in enumerate(
        (
            (tokens_hbm, tokens),
            (gain_first_hbm, gain_first),
            (gain_mixer_hbm, gain_mixer),
            (beta_hbm, beta_weight),
            (decay_hbm, decay_weight),
            (rate_hbm, decay_rate),
            (bias_hbm, decay_bias),
            (lengths_hbm, lengths),
            (head_gain_hbm, head_gain),
            (gain_second_hbm, gain_second),
        )
    ):
        small = pltpu.make_async_copy(src, dst, small_sem.at[at])
        small.start()
        smalls.append(small)

    loads = []
    for at, (src, dst) in enumerate(
        (
            (first_gate_hbm, first_gate),
            (first_up_hbm, first_up),
            (first_down_hbm, first_down),
            (query_hbm, query_w),
            (key_hbm, key_w),
            (value_hbm, value_w),
            (outgate_hbm, outgate_w),
            (state_hbm.at[0], state),
            (out_hbm, out_w),
            (second_gate_hbm, second_gate),
            (second_up_hbm, second_up),
            (second_down_hbm, second_down),
        )
    ):
        load = pltpu.make_async_copy(src, dst, load_sem.at[at])
        load.start()
        loads.append(load)

    spread_rows, half = 2 * rows, NEW
    at_row = lax.broadcasted_iota(jnp.int32, (spread_rows, rows), 0)
    at_col = lax.broadcasted_iota(jnp.int32, (spread_rows, rows), 1)
    source = (at_row // (2 * half)) * half + at_row % half
    top = (at_row % (2 * half)) < half
    hit = source == at_col
    spread_top[...] = jnp.where(hit & top, 1.0, 0.0).astype(BF16)
    spread_low[...] = jnp.where(hit & jnp.logical_not(top), 1.0, 0.0).astype(BF16)

    smalls[0].wait()
    own = pl.ds(pl.multiple_of(my_tp * own_rows, own_rows), own_rows)
    arrived[own, :] = tokens[...].astype(F32)
    place_row = lax.broadcasted_iota(jnp.int32, (rows, rows), 0)
    place_col = lax.broadcasted_iota(jnp.int32, (rows, rows), 1)
    block = place_row // half
    wanted = ((block % depth) * group + block // depth) * half + place_row % half
    natural[...] = jnp.where(wanted == place_col, 1.0, 0.0).astype(BF16)
    pl.semaphore_wait(barrier, depth - 1 + group - 1 + tps - 1)

    def all_tp(src, dst, stage, part):
        def one(step, carry):
            pltpu.make_async_remote_copy(
                src_ref=src,
                dst_ref=dst,
                send_sem=pair_sem.at[0, stage],
                recv_sem=pair_sem.at[1, stage],
                device_id={"tp": lax.rem(my_tp + step, tps)},
                device_id_type=MESH,
            ).start()
            return carry

        lax.fori_loop(1, tps, one, 0)

        def settle(sem):
            def one_wait(step, carry):
                pltpu.make_async_copy(part, part, sem).wait()
                return carry

            lax.fori_loop(1, tps, one_wait, 0)

        settle(pair_sem.at[1, stage])
        settle(pair_sem.at[0, stage])

    all_tp(arrived.at[own, :], arrived.at[own, :], 0, arrived.at[pl.ds(0, own_rows), :])
    resid[...] = jnp.dot(
        natural[...], arrived[...].astype(BF16), preferred_element_type=F32
    )

    def spread(matrix_top, matrix_low):
        low = jnp.dot(spread_low[...], matrix_low, preferred_element_type=F32)
        high = jnp.dot(spread_top[...], matrix_top, preferred_element_type=F32)
        return high, low

    def norm_operand(gain):
        whole = resid[...]
        squares = jnp.sum(whole * whole, axis=1, keepdims=True)
        operand = (whole * gain[...]).astype(BF16)
        squares_top = squares.astype(BF16)
        squares_low = (squares - squares_top.astype(F32)).astype(BF16)
        high, low = spread(operand, operand)
        sq_high, sq_low = spread(
            jnp.broadcast_to(squares_top.astype(F32), (rows, LANES)).astype(BF16),
            jnp.broadcast_to(squares_low.astype(F32), (rows, LANES)).astype(BF16),
        )
        return high.astype(BF16), low.astype(BF16), sq_high + sq_low

    def rs_first(bufs, sems, c, start, size, swapped):
        send, mid, _, _, swap_mid, _, _, _, _, _ = bufs
        cols = pl.ds(start, size)
        stage = sems // 6
        if paired and not swapped and c == 0:

            @pl.when(late)
            def _():
                pl.semaphore_wait(turn_sem.at[stage], 1)

        if swapped:
            count, place, sem = depth, my_depth, sems + 4
        else:
            count, place, sem = group, my_plane, sems

        def source(to):
            return send.at[:, to, :, cols] if swapped else send.at[to, :, :, cols]

        early = not swapped and c == early_of(bufs[8])
        target = swap_mid.at[place] if swapped else mid.at[place, :, :, cols]
        pltpu.make_async_copy(source(place), target, recv_sem.at[sems, c]).start()

        def one(step, carry):
            to = lax.rem(place + step, count)
            kv = to * group + my_plane if swapped else my_depth * group + to
            pltpu.make_async_remote_copy(
                src_ref=source(to),
                dst_ref=target,
                send_sem=early_sem.at[stage] if early else send_sem.at[sem],
                recv_sem=recv_sem.at[sems, c],
                device_id={"kv": kv},
                device_id_type=MESH,
            ).start()
            return carry

        lax.fori_loop(1, count, one, 0)

    def early_part(bufs, start, size):
        return bufs[1].at[pl.ds(0, group - 1), :, :, pl.ds(start, size)]

    def hand_over(bufs, sems, start, size):
        part = early_part(bufs, start, size)
        pltpu.make_async_copy(part, part, early_sem.at[sems // 6]).wait()
        if paired:

            @pl.when(jnp.logical_not(late))
            def _():
                pl.semaphore_signal(
                    turn_sem.at[sems // 6], inc=1, device_id={"tp": partner}, device_id_type=MESH
                )

    def rs_second(bufs, sems, c, start, size, swapped):
        _, mid, red, fin, swap_mid, swap_red, swap_fin, _, _, _ = bufs
        if swapped:
            came, kept, last, base = swap_mid, swap_red, swap_fin, 0
            count, place, sem = group, my_plane, sems + 5
        else:
            came, kept, last, base = mid, red, fin, start
            count, place, sem = depth, my_depth, sems + 1
        cols = pl.ds(base, size)
        part = came.at[:, :, :, cols]
        pltpu.make_async_copy(part, part, recv_sem.at[sems, c]).wait()
        for d in range(count):
            for at, wide in chunks_of(size, 512):
                span_at = slice(base + at, base + at + wide)
                value = came[0, d, :, span_at].astype(F32)
                for g in range(1, came.shape[0]):
                    value = value + came[g, d, :, span_at].astype(F32)
                kept[d, :, span_at] = value.astype(BF16)
        pltpu.make_async_copy(
            kept.at[place, :, cols], last.at[place, :, cols], recv_sem.at[sems + 1, c]
        ).start()

        def one(step, carry):
            to = lax.rem(place + step, count)
            kv = my_depth * group + to if swapped else to * group + my_plane
            pltpu.make_async_remote_copy(
                src_ref=kept.at[to, :, cols],
                dst_ref=last.at[place, :, cols],
                send_sem=send_sem.at[sem],
                recv_sem=recv_sem.at[sems + 1, c],
                device_id={"kv": kv},
                device_id_type=MESH,
            ).start()
            return carry

        lax.fori_loop(1, count, one, 0)

    def rs_wait(bufs, sems, c, start, size, swapped):
        part = bufs[6] if swapped else bufs[3].at[:, :, pl.ds(start, size)]
        pltpu.make_async_copy(part, part, recv_sem.at[sems + 1, c]).wait()

    def ag_depth(bufs, sems, c, start, size):
        buffer = bufs[7]
        mine = buffer.at[my_plane, my_depth, :, pl.ds(start, size)]

        def one(step, carry):
            pltpu.make_async_remote_copy(
                src_ref=mine,
                dst_ref=mine,
                send_sem=send_sem.at[sems + 2],
                recv_sem=recv_sem.at[sems + 2, c],
                device_id={"kv": lax.rem(my_depth + step, depth) * group + my_plane},
                device_id_type=MESH,
            ).start()
            return carry

        lax.fori_loop(1, depth, one, 0)

    def ag_direct(bufs, sems, c, start, size):
        buffer = bufs[7]
        mine = buffer.at[my_plane, my_depth, :, pl.ds(start, size)]

        def one(step, carry):
            far, across = step // (group - 1), 1 + lax.rem(step, group - 1)
            to_depth = lax.rem(my_depth + 1 + far, depth)
            to_plane = lax.rem(my_plane + across, group)
            pltpu.make_async_remote_copy(
                src_ref=mine,
                dst_ref=mine,
                send_sem=send_sem.at[sems + 3],
                recv_sem=recv_sem.at[sems + 3, c],
                device_id={"kv": to_depth * group + to_plane},
                device_id_type=MESH,
            ).start()
            return carry

        lax.fori_loop(0, depth * (group - 1), one, 0)

    def ag_plane(bufs, sems, c, start, size):
        buffer = bufs[7]
        cols = pl.ds(start, size)
        mine = buffer.at[my_plane, :, :, cols]

        def one(step, carry):
            pltpu.make_async_remote_copy(
                src_ref=mine,
                dst_ref=mine,
                send_sem=send_sem.at[sems + 3],
                recv_sem=recv_sem.at[sems + 3, c],
                device_id={"kv": my_depth * group + lax.rem(my_plane + step, group)},
                device_id_type=MESH,
            ).start()
            return carry

        lax.fori_loop(1, group, one, 0)

    def ag_near(bufs, sems, c, start, size):
        part = bufs[7].at[0, pl.ds(0, depth - 1), :, pl.ds(start, size)]
        pltpu.make_async_copy(part, part, recv_sem.at[sems + 2, c]).wait()

    def ag_wait(bufs, sems, c, start, size):
        part = bufs[7].at[pl.ds(0, group - 1), :, :, pl.ds(start, size)]
        pltpu.make_async_copy(part, part, recv_sem.at[sems + 3, c]).wait()

    def all_sent(bufs, sems):
        send, mid, red, fin, swap_mid, swap_red, swap_fin, buffer, _, width = bufs
        parts = [
            mid.at[pl.ds(0, group - 1), :, :, pl.ds(0, mid.shape[3] - width)],
            fin.at[pl.ds(0, depth - 1)],
            buffer.at[0, pl.ds(0, depth - 1)],
            buffer.at[pl.ds(0, group - 1)],
        ]
        if mid.shape[3] < send.shape[3]:
            parts += [swap_mid.at[pl.ds(0, depth - 1)], swap_fin.at[pl.ds(0, group - 1)]]
        for at, part in enumerate(parts):
            if min(part.shape) > 0:
                pltpu.make_async_copy(part, part, send_sem.at[sems + at]).wait()

    def put(send, start, size, value):
        send[:, :, :, start : start + size] = value.reshape(group, depth, 2 * half, size).astype(
            BF16
        )

    def total(bufs, start, size):
        fin, begin = bufs[3], start
        if start >= fin.shape[2]:
            fin, begin = bufs[6], start - fin.shape[2]
        value = fin[0, :, begin : begin + size].astype(F32)
        for k in range(1, fin.shape[0]):
            value = value + fin[k, :, begin : begin + size].astype(F32)
        return value

    def inverse_rms(bufs):
        squares = total(bufs, 0, LANES)
        return lax.rsqrt((squares[:half] + squares[half:]) / model + EPS)

    def stacked(buffer, start, size):
        flat = buffer[:, :, :, start : start + size].astype(F32).reshape(rows, size)
        return flat.astype(BF16)

    def in_order(count):
        order = list(range(count))
        if swaps(count):
            order = order[: count - 2] + [count - 1, count - 2]
        return [(stage, c) for stage in range(4) for c in order]

    def last_of(count, most):
        return [c for _, c in in_order(count)][:count][max(0, count - most) :]

    def in_issue(count):
        order = list(range(count))
        return order[-1:] + order[:-1] if swaps(count) else order

    def feed_forward(before, gain, gate, up, down, waits, bufs, pair, sems, tp_sems):
        send, hidden = bufs[0], bufs[7]
        for ready in before:
            ready.wait()
        high, low, squares = norm_operand(gain)
        units = gate.shape[1]
        count = pieces(units // LANES, 4)
        size = units // count
        put(send, 0, LANES, squares)
        waits[0].wait()
        waits[1].wait()

        def sums_at(c):
            swapped = swaps(count) and c == count - 1
            return (0, LANES + size, False) if c == 0 else (LANES + c * size, size, swapped)

        for c in in_issue(count):
            for at, wide in chunks_of(size, 512):
                lo = c * size + at
                put(
                    send,
                    LANES + lo,
                    wide,
                    jnp.dot(high, gate[:, lo : lo + wide], preferred_element_type=F32)
                    + jnp.dot(low, up[:, lo : lo + wide], preferred_element_type=F32),
                )
            rs_first(bufs, sems, c, *sums_at(c))
        hand_over(bufs, sems, *sums_at(early_of(count))[:2])
        branch = jnp.zeros((rows, width), F32)
        direct = last_of(count, HALF_DIRECT)
        scale, down_ready = None, []
        for stage, c in in_order(count):
            if stage == 0:
                rs_second(bufs, sems, c, *sums_at(c))
            elif stage == 1:
                rs_wait(bufs, sems, c, *sums_at(c))
                if c == 0:
                    scale = inverse_rms(bufs)
                for at, wide in chunks_of(size, LANES):
                    lo = c * size + at
                    both = total(bufs, LANES + lo, wide)
                    hidden[my_plane, my_depth, :, lo : lo + wide] = (
                        silu(both[:half] * scale) * (both[half:] * scale)
                    ).astype(BF16)
                ag_depth(bufs, sems, c, c * size, size)
                if c in direct:
                    ag_direct(bufs, sems, c, c * size, size)
            elif stage == 2:
                if c not in direct:
                    ag_near(bufs, sems, c, c * size, size)
                    ag_plane(bufs, sems, c, c * size, size)
            else:
                if c in direct:
                    ag_near(bufs, sems, c, c * size, size)
                ag_wait(bufs, sems, c, c * size, size)
                if not down_ready:
                    down_ready.append(waits[2].wait())
                branch = branch + jnp.dot(
                    stacked(hidden, c * size, size),
                    down[c * size : (c + 1) * size, :],
                    preferred_element_type=F32,
                )
        pair[my_tp] = branch
        all_tp(pair.at[my_tp], pair.at[my_tp], tp_sems, pair.at[0])
        branch = pair[0]
        for t in range(1, tps):
            branch = branch + pair[t]
        resid[...] = (resid[...] + 0.5 * branch).astype(BF16).astype(F32)

    half_count = pieces(first_gate.shape[1] // LANES, 4)
    half_size = first_gate.shape[1] // half_count
    mixer_count = pieces(heads, 4)
    mixer_size = 2 * heads * HEAD_DIM // mixer_count

    def early_width(before, parts, each):
        return each if early_of(parts) else before + each

    half_early = (half_count, early_width(LANES, half_count, half_size))
    mixer_early = (mixer_count, early_width(2 * LANES, mixer_count, mixer_size))
    first_bufs = (*first_sums, hidden_first, *half_early)
    mixer_bufs = (*mixer_sums, hidden_mixer, *mixer_early)
    second_bufs = (*second_sums, hidden_second, *half_early)
    send_mixer = mixer_sums[0]
    feed_forward(
        smalls[1:2], gain_first, first_gate, first_up, first_down, loads[0:3],
        first_bufs, pair_first, 0, 1,
    )

    for small in smalls[2:9]:
        small.wait()
    high, low, squares = norm_operand(gain_mixer)
    all_heads = beta_weight.shape[0]
    across = (((1,), (1,)), ((), ()))
    put(send_mixer, 0, LANES, squares)
    send_mixer[:, :, :, LANES : 2 * LANES] = jnp.zeros((group, depth, 2 * half, LANES), BF16)
    small = lax.dot_general(
        high, beta_weight[...], across, preferred_element_type=F32
    ) + lax.dot_general(low, decay_weight[...], across, preferred_element_type=F32)
    put(send_mixer, LANES, all_heads, small)
    for load in loads[3:7]:
        load.wait()
    count = pieces(heads, 4)
    batch = heads // count
    size = batch * HEAD_DIM

    def mixed_at(c):
        start = 2 * LANES + 2 * c * size
        swapped = swaps(count) and c == count - 1
        return (0, 2 * LANES + 2 * size, False) if c == 0 else (start, 2 * size, swapped)

    for c in in_issue(count):
        for at, (first, second) in enumerate(((query_w, value_w), (key_w, outgate_w))):
            lo = c * size
            put(
                send_mixer,
                2 * LANES + (2 * c + at) * size,
                size,
                jnp.dot(high, first[:, lo : lo + size], preferred_element_type=F32)
                + jnp.dot(low, second[:, lo : lo + size], preferred_element_type=F32),
            )
        rs_first(mixer_bufs, 6, c, *mixed_at(c))
    hand_over(mixer_bufs, 6, *mixed_at(early_of(count))[:2])
    lane = lax.broadcasted_iota(jnp.int32, (half, LANES), 1)
    slot = lax.broadcasted_iota(jnp.int32, (half, LANES), 0)
    live = jnp.where(slot < lengths[0], 1.0, 0.0)
    scale, logits = None, None
    direct = last_of(count, MIXER_DIRECT)
    branch = jnp.zeros((rows, width), F32)
    for stage, c in in_order(count):
        if stage == 0:
            rs_second(mixer_bufs, 6, c, *mixed_at(c))
            continue
        if stage == 2:
            if c not in direct:
                ag_near(mixer_bufs, 6, c, c * size, size)
                ag_plane(mixer_bufs, 6, c, c * size, size)
            continue
        if stage == 3:
            if c in direct:
                ag_near(mixer_bufs, 6, c, c * size, size)
            ag_wait(mixer_bufs, 6, c, c * size, size)
            if c == 0:
                loads[8].wait()
            branch = branch + jnp.dot(
                stacked(hidden_mixer, c * size, size),
                out_w[c * size : (c + 1) * size, :],
                preferred_element_type=F32,
            )
            continue
        rs_wait(mixer_bufs, 6, c, *mixed_at(c))
        if c == 0:
            scale = inverse_rms(mixer_bufs)
            logits = total(mixer_bufs, LANES, LANES)
            loads[7].wait()
        for h in range(c * batch, (c + 1) * batch):
            base = 2 * LANES + 2 * c * size + (h - c * batch) * HEAD_DIM
            both = total(mixer_bufs, base, HEAD_DIM)
            query, value = silu(both[:half] * scale), silu(both[half:] * scale)
            both = total(mixer_bufs, base + size, HEAD_DIM)
            keyvec, outgate = silu(both[:half] * scale), silu(both[half:] * scale)
            query = query * lax.rsqrt(jnp.sum(query * query, axis=1, keepdims=True) + EPS)
            query = query * HEAD_DIM ** (-0.5)
            keyvec = keyvec * lax.rsqrt(jnp.sum(keyvec * keyvec, axis=1, keepdims=True) + EPS)
            mine = lane == my_tp * heads + h
            beta_logit = jnp.sum(jnp.where(mine, logits[:half] * scale, 0.0), axis=1, keepdims=True)
            decay_logit = jnp.sum(jnp.where(mine, logits[half:] * scale, 0.0), axis=1, keepdims=True)
            beta_logit = jnp.broadcast_to(beta_logit, (half, LANES))
            decay_logit = jnp.broadcast_to(decay_logit, (half, LANES)) + decay_bias[0, h]
            beta = live / (1.0 + jnp.exp(-beta_logit))
            soft = jnp.maximum(decay_logit, 0.0) + jnp.log(1.0 + jnp.exp(-jnp.abs(decay_logit)))
            decay = -decay_rate[0, h] * soft * live
            reach = jnp.zeros_like(decay)
            for i in range(NEW):
                reach = reach + jnp.where(slot >= i, decay[i : i + 1], 0.0)
            before = jnp.exp(reach)
            old = state[h]
            held = jnp.dot(
                jnp.concatenate([keyvec, query], axis=0),
                old,
                precision=lax.Precision.HIGHEST,
                preferred_element_type=F32,
            )
            update = beta * (value - before * held[:half])
            output = before * held[half:]
            for i in range(NEW):
                between = jnp.where(slot >= i, jnp.exp(jnp.minimum(reach - reach[i : i + 1], 0.0)), 0.0)
                row = keyvec[i : i + 1]
                alike = jnp.sum(keyvec * row, axis=1, keepdims=True)
                fixed = update[i : i + 1]
                update = update - jnp.where(slot > i, beta * between * alike * fixed, 0.0)
                output = output + between * jnp.sum(query * row, axis=1, keepdims=True) * fixed
            last = reach[NEW - 1 : NEW]
            gained = update * jnp.exp(last - reach)
            zero = jnp.zeros_like(keyvec)
            new_state[0, h] = old * jnp.exp(last) + lax.dot_general(
                jnp.concatenate([keyvec, zero], axis=0),
                jnp.concatenate([gained, zero], axis=0),
                (((0,), (0,)), ((), ())),
                precision=lax.Precision.HIGHEST,
                preferred_element_type=F32,
            )
            output = output * live
            output = output * lax.rsqrt(jnp.mean(output * output, axis=1, keepdims=True) + EPS)
            output = output * head_gain[...] * outgate
            hidden_mixer[my_plane, my_depth, :, h * HEAD_DIM : (h + 1) * HEAD_DIM] = output.astype(
                BF16
            )
        ag_depth(mixer_bufs, 6, c, c * size, size)
        if c in direct:
            ag_direct(mixer_bufs, 6, c, c * size, size)
    pair_mixer[my_tp] = branch
    all_tp(pair_mixer.at[my_tp], pair_mixer.at[my_tp], 2, pair_mixer.at[0])
    branch = pair_mixer[0]
    for t in range(1, tps):
        branch = branch + pair_mixer[t]
    resid[...] = (resid[...] + branch).astype(BF16).astype(F32)

    feed_forward(
        smalls[9:10], gain_second, second_gate, second_up, second_down, loads[9:12],
        second_bufs, pair_second, 12, 3,
    )
    arrived[...] = lax.dot_general(
        natural[...], resid[...].astype(BF16), (((0,), (0,)), ((), ())), preferred_element_type=F32
    )
    layer_out[...] = arrived[own, :].astype(BF16)
    all_sent(first_bufs, 0)
    all_sent(mixer_bufs, 6)
    all_sent(second_bufs, 12)


def solution(mesh):
    n, tps = mesh.shape["kv"], mesh.shape["tp"]

    def on_device(
        tokens,
        lengths,
        memory_state,
        gain_first,
        first_gate,
        first_up,
        first_down,
        gain_mixer,
        query_weight,
        key_weight,
        value_weight,
        outgate_weight,
        beta_weight,
        decay_weight,
        decay_rate,
        decay_bias,
        head_gain,
        out_weight,
        gain_second,
        second_gate,
        second_up,
        second_down,
    ):
        rows = tokens.shape[0] * tps
        width = tokens.shape[1]
        units = first_gate.shape[1]
        span = query_weight.shape[1]
        group = pieces(n, 4)
        depth = n // group
        half_parts = pieces(units // LANES, 4)
        mixer_parts = pieces(memory_state.shape[1], 4)
        vmem = pl.BlockSpec(memory_space=pltpu.VMEM)
        hbm = pl.BlockSpec(memory_space=pltpu.HBM)

        def like(array):
            return pltpu.VMEM(array.shape, array.dtype)

        def owners(before, parts, each):
            last = each if swaps(parts) else LANES
            columns = before + parts * each
            kept = columns - (last if swaps(parts) else 0)
            return (
                pltpu.VMEM((group, depth, 2 * NEW, columns), BF16),
                pltpu.VMEM((group, depth, 2 * NEW, kept), BF16),
                pltpu.VMEM((depth, 2 * NEW, kept), BF16),
                pltpu.VMEM((depth, 2 * NEW, kept), BF16),
                pltpu.VMEM((depth, group, 2 * NEW, last), BF16),
                pltpu.VMEM((group, 2 * NEW, last), BF16),
                pltpu.VMEM((group, 2 * NEW, last), BF16),
            )

        def gathered(columns):
            return pltpu.VMEM((group, depth, NEW, columns), BF16)

        def pairs():
            return pltpu.VMEM((tps, rows, width), F32)

        parts = pl.pallas_call(
            functools.partial(layer_kernel, n, tps),
            name="layer",
            out_shape=(
                pltpu.VMEM(tokens.shape, BF16),
                pltpu.VMEM(memory_state.shape, F32),
            ),
            in_specs=[hbm] * 22,
            out_specs=(vmem, vmem),
            scratch_shapes=[
                like(tokens),
                pltpu.SMEM(lengths.shape, lengths.dtype),
                pltpu.VMEM((1, width), F32),
                pltpu.VMEM((1, width), F32),
                pltpu.VMEM(beta_weight.shape[::-1], BF16),
                pltpu.VMEM(decay_weight.shape[::-1], BF16),
                pltpu.SMEM((1, decay_rate.shape[0]), F32),
                pltpu.SMEM((1, decay_bias.shape[0]), F32),
                pltpu.VMEM((1, HEAD_DIM), F32),
                pltpu.VMEM((1, width), F32),
                like(first_gate),
                like(first_up),
                like(first_down),
                like(query_weight),
                like(key_weight),
                like(value_weight),
                like(outgate_weight),
                like(out_weight),
                like(second_gate),
                like(second_up),
                like(second_down),
                pltpu.VMEM(memory_state.shape[1:], F32),
                pltpu.VMEM((rows, width), F32),
                pltpu.VMEM((2 * rows, rows), BF16),
                pltpu.VMEM((2 * rows, rows), BF16),
                pltpu.VMEM((rows, width), F32),
                pltpu.VMEM((rows, rows), BF16),
                owners(LANES, half_parts, units // half_parts),
                owners(2 * LANES, mixer_parts, 2 * span // mixer_parts),
                owners(LANES, half_parts, units // half_parts),
                gathered(units),
                gathered(span),
                gathered(units),
                pairs(),
                pairs(),
                pairs(),
                pltpu.SemaphoreType.DMA((12,)),
                pltpu.SemaphoreType.DMA((18,)),
                pltpu.SemaphoreType.DMA((18, 4)),
                pltpu.SemaphoreType.DMA((2, 4)),
                pltpu.SemaphoreType.DMA((3,)),
                pltpu.SemaphoreType.REGULAR((3,)),
                pltpu.SemaphoreType.DMA((10,)),
            ],
            compiler_params=pltpu.CompilerParams(
                collective_id=0,
                has_side_effects=True,
                vmem_limit_bytes=60 * 1024 * 1024,
            ),
        )(
            tokens,
            lengths,
            memory_state,
            gain_first.reshape(1, -1),
            first_gate,
            first_up,
            first_down,
            gain_mixer.reshape(1, -1),
            query_weight,
            key_weight,
            value_weight,
            outgate_weight,
            beta_weight.T,
            decay_weight.T,
            decay_rate.reshape(1, -1),
            decay_bias.reshape(1, -1),
            head_gain.reshape(1, -1),
            out_weight,
            gain_second.reshape(1, -1),
            second_gate,
            second_up,
            second_down,
        )
        return pl.pallas_call(
            put_out,
            name="put_out",
            out_shape=(
                jax.ShapeDtypeStruct(tokens.shape, BF16),
                jax.ShapeDtypeStruct(memory_state.shape, F32),
            ),
            in_specs=[vmem, vmem],
            out_specs=(hbm, hbm),
            scratch_shapes=[pltpu.SemaphoreType.DMA((2,))],
            compiler_params=pltpu.CompilerParams(vmem_limit_bytes=2 * 1024 * 1024),
        )(*parts)

    in_specs = (
        P("tp", "kv"),
        P("kv"),
        P("kv", "tp", None, None),
        P("kv"),
        P("kv", "tp"),
        P("kv", "tp"),
        P("tp", "kv"),
        P("kv"),
        P("kv", "tp"),
        P("kv", "tp"),
        P("kv", "tp"),
        P("kv", "tp"),
        P("kv", None),
        P("kv", None),
        P("tp"),
        P("tp"),
        P(),
        P("tp", "kv"),
        P("kv"),
        P("kv", "tp"),
        P("kv", "tp"),
        P("tp", "kv"),
    )
    out_specs = (P("tp", "kv"), P("kv", "tp", None, None))
    return jax.shard_map(
        on_device, mesh=mesh, in_specs=in_specs, out_specs=out_specs, check_vma=False
    )
```

```python
import functools

import jax
import jax.numpy as jnp
from jax import lax
from jax.experimental import pallas as pl
from jax.experimental.pallas import tpu as pltpu
from jax.sharding import PartitionSpec as P

MESH = pl.DeviceIdType.MESH
HEAD_DIM = 128
LANES = 128
NEW = 4
EPS = 1e-06
EARLY = 1
HALF_DIRECT = 2
F32 = jnp.float32
BF16 = jnp.bfloat16


def silu(x):
    return x / (1.0 + jnp.exp(-x))


def pieces(total, most):
    return next(k for k in range(most, 0, -1) if total % k == 0)


def swaps(count):
    return count > 2


def early_of(count):
    return min(EARLY, count - 1 - int(swaps(count)))


def chunks_of(total, step):
    return [(c, min(step, total - c)) for c in range(0, total, step)]


def put_out(layer, state, layer_hbm, state_hbm, sem):
    moves = [
        pltpu.make_async_copy(src, dst, sem.at[at])
        for at, (src, dst) in enumerate(((layer, layer_hbm), (state, state_hbm)))
    ]
    for move in moves:
        move.start()
    for move in moves:
        move.wait()


def layer_kernel(
    n,
    tps,
    tokens_hbm,
    lengths_hbm,
    state_hbm,
    gain_first_hbm,
    first_gate_hbm,
    first_up_hbm,
    first_down_hbm,
    gain_mixer_hbm,
    query_hbm,
    key_hbm,
    value_hbm,
    outgate_hbm,
    beta_hbm,
    decay_hbm,
    rate_hbm,
    bias_hbm,
    head_gain_hbm,
    out_hbm,
    gain_second_hbm,
    second_gate_hbm,
    second_up_hbm,
    second_down_hbm,
    layer_out,
    new_state,
    tokens,
    lengths,
    gain_first,
    gain_mixer,
    beta_weight,
    decay_weight,
    decay_rate,
    decay_bias,
    head_gain,
    gain_second,
    first_gate,
    first_up,
    first_down,
    query_w,
    key_w,
    value_w,
    outgate_w,
    out_w,
    second_gate,
    second_up,
    second_down,
    state,
    split,
    resid,
    spread_top,
    spread_low,
    arrived,
    natural,
    first_sums,
    mixer_sums,
    second_sums,
    hidden_first,
    hidden_mixer,
    hidden_second,
    pair_first,
    pair_mixer,
    pair_second,
    load_sem,
    send_sem,
    recv_sem,
    pair_sem,
    early_sem,
    turn_sem,
    small_sem,
):
    me = lax.axis_index("kv")
    my_tp = lax.axis_index("tp")
    rows, width = resid.shape
    own_rows = rows // tps
    group = hidden_first.shape[0]
    depth = n // group
    my_plane, my_depth = lax.rem(me, group), me // group
    heads = state.shape[0]
    model = n * width
    paired = tps % 2 == 0
    late = lax.rem(my_tp, 2) == 1
    partner = my_tp + 1 - 2 * lax.rem(my_tp, 2)

    barrier = pltpu.get_barrier_semaphore()

    def greet_plane(step, carry):
        to = my_depth * group + lax.rem(my_plane + step, group)
        pl.semaphore_signal(barrier, inc=1, device_id={"kv": to}, device_id_type=MESH)
        return carry

    def greet_depth(step, carry):
        to = lax.rem(my_depth + step, depth) * group + my_plane
        pl.semaphore_signal(barrier, inc=1, device_id={"kv": to}, device_id_type=MESH)
        return carry

    def greet_tp(step, carry):
        pl.semaphore_signal(
            barrier, inc=1, device_id={"tp": lax.rem(my_tp + step, tps)}, device_id_type=MESH
        )
        return carry

    lax.fori_loop(1, depth, greet_depth, 0)
    lax.fori_loop(1, group, greet_plane, 0)
    lax.fori_loop(1, tps, greet_tp, 0)

    smalls = []
    for at, (src, dst) in enumerate(
        (
            (tokens_hbm, tokens),
            (gain_first_hbm, gain_first),
            (gain_mixer_hbm, gain_mixer),
            (beta_hbm, beta_weight),
            (decay_hbm, decay_weight),
            (rate_hbm, decay_rate),
            (bias_hbm, decay_bias),
            (lengths_hbm, lengths),
            (head_gain_hbm, head_gain),
            (gain_second_hbm, gain_second),
        )
    ):
        small = pltpu.make_async_copy(src, dst, small_sem.at[at])
        small.start()
        smalls.append(small)

    loads = []
    for at, (src, dst) in enumerate(
        (
            (first_gate_hbm, first_gate),
            (first_up_hbm, first_up),
            (first_down_hbm, first_down),
            (query_hbm, query_w),
            (key_hbm, key_w),
            (value_hbm, value_w),
            (outgate_hbm, outgate_w),
            (state_hbm.at[0], state),
            (out_hbm, out_w),
            (second_gate_hbm, second_gate),
            (second_up_hbm, second_up),
            (second_down_hbm, second_down),
        )
    ):
        load = pltpu.make_async_copy(src, dst, load_sem.at[at])
        load.start()
        loads.append(load)

    spread_rows, half = 2 * rows, NEW
    at_row = lax.broadcasted_iota(jnp.int32, (spread_rows, rows), 0)
    at_col = lax.broadcasted_iota(jnp.int32, (spread_rows, rows), 1)
    source = (at_row // (2 * half)) * half + at_row % half
    top = (at_row % (2 * half)) < half
    hit = source == at_col
    spread_top[...] = jnp.where(hit & top, 1.0, 0.0).astype(BF16)
    spread_low[...] = jnp.where(hit & jnp.logical_not(top), 1.0, 0.0).astype(BF16)

    smalls[0].wait()
    own = pl.ds(pl.multiple_of(my_tp * own_rows, own_rows), own_rows)
    arrived[own, :] = tokens[...].astype(F32)
    place_row = lax.broadcasted_iota(jnp.int32, (rows, rows), 0)
    place_col = lax.broadcasted_iota(jnp.int32, (rows, rows), 1)
    block = place_row // half
    wanted = ((block % depth) * group + block // depth) * half + place_row % half
    natural[...] = jnp.where(wanted == place_col, 1.0, 0.0).astype(BF16)
    pl.semaphore_wait(barrier, depth - 1 + group - 1 + tps - 1)

    def all_tp(src, dst, stage, part):
        def one(step, carry):
            pltpu.make_async_remote_copy(
                src_ref=src,
                dst_ref=dst,
                send_sem=pair_sem.at[0, stage],
                recv_sem=pair_sem.at[1, stage],
                device_id={"tp": lax.rem(my_tp + step, tps)},
                device_id_type=MESH,
            ).start()
            return carry

        lax.fori_loop(1, tps, one, 0)

        def settle(sem):
            def one_wait(step, carry):
                pltpu.make_async_copy(part, part, sem).wait()
                return carry

            lax.fori_loop(1, tps, one_wait, 0)

        settle(pair_sem.at[1, stage])
        settle(pair_sem.at[0, stage])

    all_tp(arrived.at[own, :], arrived.at[own, :], 0, arrived.at[pl.ds(0, own_rows), :])
    resid[...] = jnp.dot(
        natural[...], arrived[...].astype(BF16), preferred_element_type=F32
    )

    def spread(matrix_top, matrix_low):
        low = jnp.dot(spread_low[...], matrix_low, preferred_element_type=F32)
        high = jnp.dot(spread_top[...], matrix_top, preferred_element_type=F32)
        return high, low

    def norm_operand(gain):
        whole = resid[...]
        squares = jnp.sum(whole * whole, axis=1, keepdims=True)
        operand = (whole * gain[...]).astype(BF16)
        squares_top = squares.astype(BF16)
        squares_low = (squares - squares_top.astype(F32)).astype(BF16)
        high, low = spread(operand, operand)
        sq_high, sq_low = spread(
            jnp.broadcast_to(squares_top.astype(F32), (rows, LANES)).astype(BF16),
            jnp.broadcast_to(squares_low.astype(F32), (rows, LANES)).astype(BF16),
        )
        return high.astype(BF16), low.astype(BF16), sq_high + sq_low

    def rs_first(bufs, sems, c, start, size, swapped):
        send, mid, _, _, swap_mid, _, _, _, _, _ = bufs
        cols = pl.ds(start, size)
        stage = sems // 6
        if swapped:
            count, place, sem = depth, my_depth, sems + 4
        else:
            count, place, sem = group, my_plane, sems

        def source(to):
            return send.at[:, to, :, cols] if swapped else send.at[to, :, :, cols]

        early = not swapped and c == early_of(bufs[8])
        target = swap_mid.at[place] if swapped else mid.at[place, :, :, cols]
        pltpu.make_async_copy(source(place), target, recv_sem.at[sems, c]).start()

        def one(step, carry):
            to = lax.rem(place + step, count)
            kv = to * group + my_plane if swapped else my_depth * group + to
            pltpu.make_async_remote_copy(
                src_ref=source(to),
                dst_ref=target,
                send_sem=early_sem.at[stage] if early else send_sem.at[sem],
                recv_sem=recv_sem.at[sems, c],
                device_id={"kv": kv},
                device_id_type=MESH,
            ).start()
            return carry

        lax.fori_loop(1, count, one, 0)

    def early_part(bufs, start, size):
        return bufs[1].at[pl.ds(0, group - 1), :, :, pl.ds(start, size)]

    def rs_begin(bufs, sems, order, sums_at, fill):
        stage = sems // 6
        for at, c in enumerate(order):
            fill(c)
            if c:
                rs_first(bufs, sems, c, *sums_at(c))
            if not paired:
                if c == 0:
                    rs_first(bufs, sems, c, *sums_at(c))
                continue
            if c == 0:

                @pl.when(jnp.logical_not(late))
                def _():
                    rs_first(bufs, sems, 0, *sums_at(0))

            if at == min(1, len(order) - 1):

                @pl.when(late)
                def _():
                    pl.semaphore_wait(turn_sem.at[stage], 1)
                    rs_first(bufs, sems, 0, *sums_at(0))

    def hand_over(bufs, sems, start, size):
        part = early_part(bufs, start, size)
        pltpu.make_async_copy(part, part, early_sem.at[sems // 6]).wait()
        if paired:

            @pl.when(jnp.logical_not(late))
            def _():
                pl.semaphore_signal(
                    turn_sem.at[sems // 6], inc=1, device_id={"tp": partner}, device_id_type=MESH
                )

    def rs_second(bufs, sems, c, start, size, swapped):
        _, mid, red, fin, swap_mid, swap_red, swap_fin, _, _, _ = bufs
        if swapped:
            came, kept, last, base = swap_mid, swap_red, swap_fin, 0
            count, place, sem = group, my_plane, sems + 5
        else:
            came, kept, last, base = mid, red, fin, start
            count, place, sem = depth, my_depth, sems + 1
        cols = pl.ds(base, size)
        part = came.at[:, :, :, cols]
        pltpu.make_async_copy(part, part, recv_sem.at[sems, c]).wait()
        for d in range(count):
            for at, wide in chunks_of(size, 512):
                span_at = slice(base + at, base + at + wide)
                value = came[0, d, :, span_at].astype(F32)
                for g in range(1, came.shape[0]):
                    value = value + came[g, d, :, span_at].astype(F32)
                kept[d, :, span_at] = value.astype(BF16)
        pltpu.make_async_copy(
            kept.at[place, :, cols], last.at[place, :, cols], recv_sem.at[sems + 1, c]
        ).start()

        def one(step, carry):
            to = lax.rem(place + step, count)
            kv = my_depth * group + to if swapped else to * group + my_plane
            pltpu.make_async_remote_copy(
                src_ref=kept.at[to, :, cols],
                dst_ref=last.at[place, :, cols],
                send_sem=send_sem.at[sem],
                recv_sem=recv_sem.at[sems + 1, c],
                device_id={"kv": kv},
                device_id_type=MESH,
            ).start()
            return carry

        lax.fori_loop(1, count, one, 0)

    def rs_wait(bufs, sems, c, start, size, swapped):
        part = bufs[6] if swapped else bufs[3].at[:, :, pl.ds(start, size)]
        pltpu.make_async_copy(part, part, recv_sem.at[sems + 1, c]).wait()

    def ag_depth(bufs, sems, c, start, size):
        buffer = bufs[7]
        mine = buffer.at[my_plane, my_depth, :, pl.ds(start, size)]

        def one(step, carry):
            pltpu.make_async_remote_copy(
                src_ref=mine,
                dst_ref=mine,
                send_sem=send_sem.at[sems + 2],
                recv_sem=recv_sem.at[sems + 2, c],
                device_id={"kv": lax.rem(my_depth + step, depth) * group + my_plane},
                device_id_type=MESH,
            ).start()
            return carry

        lax.fori_loop(1, depth, one, 0)

    def ag_direct(bufs, sems, c, start, size):
        buffer = bufs[7]
        mine = buffer.at[my_plane, my_depth, :, pl.ds(start, size)]

        def one(step, carry):
            far, across = step // (group - 1), 1 + lax.rem(step, group - 1)
            to_depth = lax.rem(my_depth + 1 + far, depth)
            to_plane = lax.rem(my_plane + across, group)
            pltpu.make_async_remote_copy(
                src_ref=mine,
                dst_ref=mine,
                send_sem=send_sem.at[sems + 3],
                recv_sem=recv_sem.at[sems + 3, c],
                device_id={"kv": to_depth * group + to_plane},
                device_id_type=MESH,
            ).start()
            return carry

        lax.fori_loop(0, depth * (group - 1), one, 0, unroll=n <= 16)

    def ag_plane(bufs, sems, c, start, size):
        buffer = bufs[7]
        cols = pl.ds(start, size)
        mine = buffer.at[my_plane, :, :, cols]

        def one(step, carry):
            pltpu.make_async_remote_copy(
                src_ref=mine,
                dst_ref=mine,
                send_sem=send_sem.at[sems + 3],
                recv_sem=recv_sem.at[sems + 3, c],
                device_id={"kv": my_depth * group + lax.rem(my_plane + step, group)},
                device_id_type=MESH,
            ).start()
            return carry

        lax.fori_loop(1, group, one, 0)

    def ag_near(bufs, sems, c, start, size):
        part = bufs[7].at[0, pl.ds(0, depth - 1), :, pl.ds(start, size)]
        pltpu.make_async_copy(part, part, recv_sem.at[sems + 2, c]).wait()

    def ag_wait(bufs, sems, c, start, size):
        part = bufs[7].at[pl.ds(0, group - 1), :, :, pl.ds(start, size)]
        pltpu.make_async_copy(part, part, recv_sem.at[sems + 3, c]).wait()

    def all_sent(bufs, sems):
        send, mid, red, fin, swap_mid, swap_red, swap_fin, buffer, _, width = bufs
        parts = [
            mid.at[pl.ds(0, group - 1), :, :, pl.ds(0, mid.shape[3] - width)],
            fin.at[pl.ds(0, depth - 1)],
            buffer.at[0, pl.ds(0, depth - 1)],
            buffer.at[pl.ds(0, group - 1)],
        ]
        if mid.shape[3] < send.shape[3]:
            parts += [swap_mid.at[pl.ds(0, depth - 1)], swap_fin.at[pl.ds(0, group - 1)]]
        for at, part in enumerate(parts):
            if min(part.shape) > 0:
                pltpu.make_async_copy(part, part, send_sem.at[sems + at]).wait()

    def put(send, start, size, value):
        send[:, :, :, start : start + size] = value.reshape(group, depth, 2 * half, size).astype(
            BF16
        )

    def total(bufs, start, size):
        fin, begin = bufs[3], start
        if start >= fin.shape[2]:
            fin, begin = bufs[6], start - fin.shape[2]
        value = fin[0, :, begin : begin + size].astype(F32)
        for k in range(1, fin.shape[0]):
            value = value + fin[k, :, begin : begin + size].astype(F32)
        return value

    def inverse_rms(bufs):
        squares = total(bufs, 0, LANES)
        return lax.rsqrt((squares[:half] + squares[half:]) / model + EPS)

    def stacked(buffer, start, size):
        flat = buffer[:, :, :, start : start + size].astype(F32).reshape(rows, size)
        return flat.astype(BF16)

    def in_order(count):
        order = list(range(count))
        if swaps(count):
            order = order[: count - 2] + [count - 1, count - 2]
        return [(stage, c) for stage in range(4) for c in order]

    def last_of(count, most):
        return [c for _, c in in_order(count)][:count][max(0, count - most) :]

    def in_issue(count):
        order = list(range(count))
        return order[:1] + order[-1:] + order[1:-1] if swaps(count) else order

    def feed_forward(before, gain, gate, up, down, waits, bufs, pair, sems, tp_sems):
        send, hidden = bufs[0], bufs[7]
        for ready in before:
            ready.wait()
        high, low, squares = norm_operand(gain)
        units = gate.shape[1]
        count = pieces(units // LANES, 4)
        size = units // count
        put(send, 0, LANES, squares)
        waits[0].wait()
        waits[1].wait()

        def sums_at(c):
            swapped = swaps(count) and c == count - 1
            return (0, LANES + size, False) if c == 0 else (LANES + c * size, size, swapped)

        def fill(c):
            for at, wide in chunks_of(size, 512):
                lo = c * size + at
                put(
                    send,
                    LANES + lo,
                    wide,
                    jnp.dot(high, gate[:, lo : lo + wide], preferred_element_type=F32)
                    + jnp.dot(low, up[:, lo : lo + wide], preferred_element_type=F32),
                )

        rs_begin(bufs, sems, in_issue(count), sums_at, fill)
        hand_over(bufs, sems, *sums_at(early_of(count))[:2])
        branch = jnp.zeros((rows, width), F32)
        direct = last_of(count, HALF_DIRECT)
        scale, down_ready = None, []
        for stage, c in in_order(count):
            if stage == 0:
                rs_second(bufs, sems, c, *sums_at(c))
            elif stage == 1:
                rs_wait(bufs, sems, c, *sums_at(c))
                if c == 0:
                    scale = inverse_rms(bufs)
                for at, wide in chunks_of(size, LANES):
                    lo = c * size + at
                    both = total(bufs, LANES + lo, wide)
                    hidden[my_plane, my_depth, :, lo : lo + wide] = (
                        silu(both[:half] * scale) * (both[half:] * scale)
                    ).astype(BF16)
                ag_depth(bufs, sems, c, c * size, size)
                if c in direct:
                    ag_direct(bufs, sems, c, c * size, size)
            elif stage == 2:
                if c not in direct:
                    ag_near(bufs, sems, c, c * size, size)
                    ag_plane(bufs, sems, c, c * size, size)
            else:
                if c in direct:
                    ag_near(bufs, sems, c, c * size, size)
                ag_wait(bufs, sems, c, c * size, size)
                if not down_ready:
                    down_ready.append(waits[2].wait())
                branch = branch + jnp.dot(
                    stacked(hidden, c * size, size),
                    down[c * size : (c + 1) * size, :],
                    preferred_element_type=F32,
                )
        pair[my_tp] = branch
        all_tp(pair.at[my_tp], pair.at[my_tp], tp_sems, pair.at[0])
        branch = pair[0]
        for t in range(1, tps):
            branch = branch + pair[t]
        resid[...] = (resid[...] + 0.5 * branch).astype(BF16).astype(F32)

    half_count = pieces(first_gate.shape[1] // LANES, 4)
    half_size = first_gate.shape[1] // half_count
    mixer_count = pieces(heads, 4)
    mixer_size = 2 * heads * HEAD_DIM // mixer_count

    def early_width(before, parts, each):
        return each if early_of(parts) else before + each

    half_early = (half_count, early_width(LANES, half_count, half_size))
    mixer_early = (mixer_count, early_width(2 * LANES, mixer_count, mixer_size))
    first_bufs = (*first_sums, hidden_first, *half_early)
    mixer_bufs = (*mixer_sums, hidden_mixer, *mixer_early)
    second_bufs = (*second_sums, hidden_second, *half_early)
    send_mixer = mixer_sums[0]
    feed_forward(
        smalls[1:2], gain_first, first_gate, first_up, first_down, loads[0:3],
        first_bufs, pair_first, 0, 1,
    )

    for small in smalls[2:9]:
        small.wait()
    high, low, squares = norm_operand(gain_mixer)
    all_heads = beta_weight.shape[0]
    across = (((1,), (1,)), ((), ()))
    put(send_mixer, 0, LANES, squares)
    send_mixer[:, :, :, LANES : 2 * LANES] = jnp.zeros((group, depth, 2 * half, LANES), BF16)
    small = lax.dot_general(
        high, beta_weight[...], across, preferred_element_type=F32
    ) + lax.dot_general(low, decay_weight[...], across, preferred_element_type=F32)
    put(send_mixer, LANES, all_heads, small)
    for load in loads[3:7]:
        load.wait()
    count = pieces(heads, 4)
    batch = heads // count
    size = batch * HEAD_DIM

    def mixed_at(c):
        start = 2 * LANES + 2 * c * size
        swapped = swaps(count) and c == count - 1
        return (0, 2 * LANES + 2 * size, False) if c == 0 else (start, 2 * size, swapped)

    def fill(c):
        for at, (first, second) in enumerate(((query_w, value_w), (key_w, outgate_w))):
            lo = c * size
            put(
                send_mixer,
                2 * LANES + (2 * c + at) * size,
                size,
                jnp.dot(high, first[:, lo : lo + size], preferred_element_type=F32)
                + jnp.dot(low, second[:, lo : lo + size], preferred_element_type=F32),
            )

    rs_begin(mixer_bufs, 6, in_issue(count), mixed_at, fill)
    hand_over(mixer_bufs, 6, *mixed_at(early_of(count))[:2])
    lane = lax.broadcasted_iota(jnp.int32, (half, LANES), 1)
    slot = lax.broadcasted_iota(jnp.int32, (half, LANES), 0)
    live = jnp.where(slot < lengths[0], 1.0, 0.0)
    loads[7].wait()
    for h in range(heads):
        old = state[h]
        top = old.astype(BF16)
        split[h, :, :HEAD_DIM] = top
        split[h, :, HEAD_DIM:] = (old - top.astype(F32)).astype(BF16)
    for stage, c in in_order(count)[:count]:
        rs_second(mixer_bufs, 6, c, *mixed_at(c))
    groups = [range(c, min(c + 2, count)) for c in range(0, count, 2)]
    scale, logits, grown = None, None, []
    for group_of in groups:
        for c in group_of:
            rs_wait(mixer_bufs, 6, c, *mixed_at(c))
        if scale is None:
            scale = inverse_rms(mixer_bufs)
            logits = total(mixer_bufs, LANES, LANES)
        for h in range(group_of[0] * batch, (group_of[-1] + 1) * batch):
            c = h // batch
            base = 2 * LANES + 2 * c * size + (h - c * batch) * HEAD_DIM
            both = total(mixer_bufs, base, HEAD_DIM)
            query, value = silu(both[:half] * scale), silu(both[half:] * scale)
            both = total(mixer_bufs, base + size, HEAD_DIM)
            keyvec, outgate = silu(both[:half] * scale), silu(both[half:] * scale)
            query = query * lax.rsqrt(jnp.sum(query * query, axis=1, keepdims=True) + EPS)
            query = query * HEAD_DIM ** (-0.5)
            keyvec = keyvec * lax.rsqrt(jnp.sum(keyvec * keyvec, axis=1, keepdims=True) + EPS)
            mine = lane == my_tp * heads + h
            beta_logit = jnp.sum(jnp.where(mine, logits[:half] * scale, 0.0), axis=1, keepdims=True)
            decay_logit = jnp.sum(jnp.where(mine, logits[half:] * scale, 0.0), axis=1, keepdims=True)
            beta_logit = jnp.broadcast_to(beta_logit, (half, LANES))
            decay_logit = jnp.broadcast_to(decay_logit, (half, LANES)) + decay_bias[0, h]
            beta = live / (1.0 + jnp.exp(-beta_logit))
            soft = jnp.maximum(decay_logit, 0.0) + jnp.log(1.0 + jnp.exp(-jnp.abs(decay_logit)))
            decay = -decay_rate[0, h] * soft * live
            reach = jnp.zeros_like(decay)
            for i in range(NEW):
                reach = reach + jnp.where(slot >= i, decay[i : i + 1], 0.0)
            before = jnp.exp(reach)
            asked = jnp.concatenate([keyvec, query], axis=0)
            top = asked.astype(BF16).astype(F32)
            found = jnp.dot(
                jnp.concatenate([top, asked - top], axis=0).astype(BF16),
                split[h],
                preferred_element_type=F32,
            )
            held = (
                found[: 2 * half, :HEAD_DIM]
                + found[2 * half :, :HEAD_DIM]
                + found[: 2 * half, HEAD_DIM:]
            )
            update = beta * (value - before * held[:half])
            output = before * held[half:]
            for i in range(NEW):
                between = jnp.where(slot >= i, jnp.exp(jnp.minimum(reach - reach[i : i + 1], 0.0)), 0.0)
                row = keyvec[i : i + 1]
                alike = jnp.sum(keyvec * row, axis=1, keepdims=True)
                fixed = update[i : i + 1]
                update = update - jnp.where(slot > i, beta * between * alike * fixed, 0.0)
                output = output + between * jnp.sum(query * row, axis=1, keepdims=True) * fixed
            last = reach[NEW - 1 : NEW]
            grown.append((keyvec, update * jnp.exp(last - reach), jnp.exp(last)))
            output = output * live
            output = output * lax.rsqrt(jnp.mean(output * output, axis=1, keepdims=True) + EPS)
            output = output * head_gain[...] * outgate
            hidden_mixer[my_plane, my_depth, :, h * HEAD_DIM : (h + 1) * HEAD_DIM] = output.astype(
                BF16
            )
        part = (group_of[0], group_of[0] * size, len(group_of) * size)
        ag_depth(mixer_bufs, 6, *part)
        ag_direct(mixer_bufs, 6, *part)
    for h, (keyvec, gained, kept) in enumerate(grown):
        zero = jnp.zeros_like(keyvec)
        new_state[0, h] = state[h] * kept + lax.dot_general(
            jnp.concatenate([keyvec, zero], axis=0),
            jnp.concatenate([gained, zero], axis=0),
            (((0,), (0,)), ((), ())),
            precision=lax.Precision.HIGHEST,
            preferred_element_type=F32,
        )
    loads[8].wait()
    branch = jnp.zeros((rows, width), F32)
    for group_of in groups:
        start, wide = group_of[0] * size, len(group_of) * size
        ag_near(mixer_bufs, 6, group_of[0], start, wide)
        ag_wait(mixer_bufs, 6, group_of[0], start, wide)
        branch = branch + jnp.dot(
            stacked(hidden_mixer, start, wide),
            out_w[start : start + wide, :],
            preferred_element_type=F32,
        )
    pair_mixer[my_tp] = branch
    all_tp(pair_mixer.at[my_tp], pair_mixer.at[my_tp], 2, pair_mixer.at[0])
    branch = pair_mixer[0]
    for t in range(1, tps):
        branch = branch + pair_mixer[t]
    resid[...] = (resid[...] + branch).astype(BF16).astype(F32)

    feed_forward(
        smalls[9:10], gain_second, second_gate, second_up, second_down, loads[9:12],
        second_bufs, pair_second, 12, 3,
    )
    arrived[...] = lax.dot_general(
        natural[...], resid[...].astype(BF16), (((0,), (0,)), ((), ())), preferred_element_type=F32
    )
    layer_out[...] = arrived[own, :].astype(BF16)
    all_sent(first_bufs, 0)
    all_sent(mixer_bufs, 6)
    all_sent(second_bufs, 12)


def solution(mesh):
    n, tps = mesh.shape["kv"], mesh.shape["tp"]

    def on_device(
        tokens,
        lengths,
        memory_state,
        gain_first,
        first_gate,
        first_up,
        first_down,
        gain_mixer,
        query_weight,
        key_weight,
        value_weight,
        outgate_weight,
        beta_weight,
        decay_weight,
        decay_rate,
        decay_bias,
        head_gain,
        out_weight,
        gain_second,
        second_gate,
        second_up,
        second_down,
    ):
        rows = tokens.shape[0] * tps
        width = tokens.shape[1]
        units = first_gate.shape[1]
        span = query_weight.shape[1]
        group = pieces(n, 4)
        depth = n // group
        half_parts = pieces(units // LANES, 4)
        mixer_parts = pieces(memory_state.shape[1], 4)
        vmem = pl.BlockSpec(memory_space=pltpu.VMEM)
        hbm = pl.BlockSpec(memory_space=pltpu.HBM)

        def like(array):
            return pltpu.VMEM(array.shape, array.dtype)

        def owners(before, parts, each):
            last = each if swaps(parts) else LANES
            columns = before + parts * each
            kept = columns - (last if swaps(parts) else 0)
            return (
                pltpu.VMEM((group, depth, 2 * NEW, columns), BF16),
                pltpu.VMEM((group, depth, 2 * NEW, kept), BF16),
                pltpu.VMEM((depth, 2 * NEW, kept), BF16),
                pltpu.VMEM((depth, 2 * NEW, kept), BF16),
                pltpu.VMEM((depth, group, 2 * NEW, last), BF16),
                pltpu.VMEM((group, 2 * NEW, last), BF16),
                pltpu.VMEM((group, 2 * NEW, last), BF16),
            )

        def gathered(columns):
            return pltpu.VMEM((group, depth, NEW, columns), BF16)

        def pairs():
            return pltpu.VMEM((tps, rows, width), F32)

        parts = pl.pallas_call(
            functools.partial(layer_kernel, n, tps),
            name="layer",
            out_shape=(
                pltpu.VMEM(tokens.shape, BF16),
                pltpu.VMEM(memory_state.shape, F32),
            ),
            in_specs=[hbm] * 22,
            out_specs=(vmem, vmem),
            scratch_shapes=[
                like(tokens),
                pltpu.SMEM(lengths.shape, lengths.dtype),
                pltpu.VMEM((1, width), F32),
                pltpu.VMEM((1, width), F32),
                pltpu.VMEM(beta_weight.shape[::-1], BF16),
                pltpu.VMEM(decay_weight.shape[::-1], BF16),
                pltpu.SMEM((1, decay_rate.shape[0]), F32),
                pltpu.SMEM((1, decay_bias.shape[0]), F32),
                pltpu.VMEM((1, HEAD_DIM), F32),
                pltpu.VMEM((1, width), F32),
                like(first_gate),
                like(first_up),
                like(first_down),
                like(query_weight),
                like(key_weight),
                like(value_weight),
                like(outgate_weight),
                like(out_weight),
                like(second_gate),
                like(second_up),
                like(second_down),
                pltpu.VMEM(memory_state.shape[1:], F32),
                pltpu.VMEM((*memory_state.shape[1:3], 2 * HEAD_DIM), BF16),
                pltpu.VMEM((rows, width), F32),
                pltpu.VMEM((2 * rows, rows), BF16),
                pltpu.VMEM((2 * rows, rows), BF16),
                pltpu.VMEM((rows, width), F32),
                pltpu.VMEM((rows, rows), BF16),
                owners(LANES, half_parts, units // half_parts),
                owners(2 * LANES, mixer_parts, 2 * span // mixer_parts),
                owners(LANES, half_parts, units // half_parts),
                gathered(units),
                gathered(span),
                gathered(units),
                pairs(),
                pairs(),
                pairs(),
                pltpu.SemaphoreType.DMA((12,)),
                pltpu.SemaphoreType.DMA((18,)),
                pltpu.SemaphoreType.DMA((18, 4)),
                pltpu.SemaphoreType.DMA((2, 4)),
                pltpu.SemaphoreType.DMA((3,)),
                pltpu.SemaphoreType.REGULAR((3,)),
                pltpu.SemaphoreType.DMA((10,)),
            ],
            compiler_params=pltpu.CompilerParams(
                collective_id=0,
                has_side_effects=True,
                vmem_limit_bytes=60 * 1024 * 1024,
            ),
        )(
            tokens,
            lengths,
            memory_state,
            gain_first.reshape(1, -1),
            first_gate,
            first_up,
            first_down,
            gain_mixer.reshape(1, -1),
            query_weight,
            key_weight,
            value_weight,
            outgate_weight,
            beta_weight.T,
            decay_weight.T,
            decay_rate.reshape(1, -1),
            decay_bias.reshape(1, -1),
            head_gain.reshape(1, -1),
            out_weight,
            gain_second.reshape(1, -1),
            second_gate,
            second_up,
            second_down,
        )
        return pl.pallas_call(
            put_out,
            name="put_out",
            out_shape=(
                jax.ShapeDtypeStruct(tokens.shape, BF16),
                jax.ShapeDtypeStruct(memory_state.shape, F32),
            ),
            in_specs=[vmem, vmem],
            out_specs=(hbm, hbm),
            scratch_shapes=[pltpu.SemaphoreType.DMA((2,))],
            compiler_params=pltpu.CompilerParams(vmem_limit_bytes=2 * 1024 * 1024),
        )(*parts)

    in_specs = (
        P("tp", "kv"),
        P("kv"),
        P("kv", "tp", None, None),
        P("kv"),
        P("kv", "tp"),
        P("kv", "tp"),
        P("tp", "kv"),
        P("kv"),
        P("kv", "tp"),
        P("kv", "tp"),
        P("kv", "tp"),
        P("kv", "tp"),
        P("kv", None),
        P("kv", None),
        P("tp"),
        P("tp"),
        P(),
        P("tp", "kv"),
        P("kv"),
        P("kv", "tp"),
        P("kv", "tp"),
        P("tp", "kv"),
    )
    out_specs = (P("tp", "kv"), P("kv", "tp", None, None))
    return jax.shard_map(
        on_device, mesh=mesh, in_specs=in_specs, out_specs=out_specs, check_vma=False
    )
```

```python
import functools

import jax
import jax.numpy as jnp
from jax import lax
from jax.experimental import pallas as pl
from jax.experimental.pallas import tpu as pltpu
from jax.sharding import PartitionSpec as P

MESH = pl.DeviceIdType.MESH
HEAD_DIM = 128
LANES = 128
NEW = 4
EPS = 1e-06
SHIFT = ((0, -1), (1, -1), (2, 2))
HEAD_CUT = 2
EARLY = 1
HALF_DIRECT = (2, 1)
F32 = jnp.float32
BF16 = jnp.bfloat16


def silu(x):
    return x / (1.0 + jnp.exp(-x))


def pieces(total, most):
    return next(k for k in range(most, 0, -1) if total % k == 0)


def swaps(count):
    return count > 2


def shares(units, count):
    tiles = units // LANES // count
    if swaps(count) and tiles > 3:
        parts = [tiles] * count
        for c, more in SHIFT:
            parts[c] += more
    else:
        parts = [tiles] * count
    return [part * LANES for part in parts]


def early_of(count):
    return min(EARLY, count - 1 - int(swaps(count)))


def chunks_of(total, step):
    return [(c, min(step, total - c)) for c in range(0, total, step)]


def put_out(layer, state, layer_hbm, state_hbm, sem):
    moves = [
        pltpu.make_async_copy(src, dst, sem.at[at])
        for at, (src, dst) in enumerate(((layer, layer_hbm), (state, state_hbm)))
    ]
    for move in moves:
        move.start()
    for move in moves:
        move.wait()


def layer_kernel(
    n,
    tps,
    tokens_hbm,
    lengths_hbm,
    state_hbm,
    gain_first_hbm,
    first_gate_hbm,
    first_up_hbm,
    first_down_hbm,
    gain_mixer_hbm,
    query_hbm,
    key_hbm,
    value_hbm,
    outgate_hbm,
    beta_hbm,
    decay_hbm,
    rate_hbm,
    bias_hbm,
    head_gain_hbm,
    out_hbm,
    gain_second_hbm,
    second_gate_hbm,
    second_up_hbm,
    second_down_hbm,
    layer_out,
    new_state,
    tokens,
    lengths,
    gain_first,
    gain_mixer,
    beta_weight,
    decay_weight,
    decay_rate,
    decay_bias,
    head_gain,
    gain_second,
    first_gate,
    first_up,
    first_down,
    query_w,
    key_w,
    value_w,
    outgate_w,
    out_w,
    second_gate,
    second_up,
    second_down,
    state,
    split,
    resid,
    spread_top,
    spread_low,
    arrived,
    natural,
    first_sums,
    mixer_sums,
    second_sums,
    hidden_first,
    hidden_mixer,
    hidden_second,
    pair_first,
    pair_mixer,
    pair_second,
    load_sem,
    send_sem,
    recv_sem,
    pair_sem,
    early_sem,
    turn_sem,
    small_sem,
):
    me = lax.axis_index("kv")
    my_tp = lax.axis_index("tp")
    rows, width = resid.shape
    own_rows = rows // tps
    group = hidden_first.shape[0]
    depth = n // group
    my_plane, my_depth = lax.rem(me, group), me // group
    heads = state.shape[0]
    model = n * width
    paired = tps % 2 == 0
    late = lax.rem(my_tp, 2) == 1
    partner = my_tp + 1 - 2 * lax.rem(my_tp, 2)

    barrier = pltpu.get_barrier_semaphore()

    def greet_plane(step, carry):
        to = my_depth * group + lax.rem(my_plane + step, group)
        pl.semaphore_signal(barrier, inc=1, device_id={"kv": to}, device_id_type=MESH)
        return carry

    def greet_depth(step, carry):
        to = lax.rem(my_depth + step, depth) * group + my_plane
        pl.semaphore_signal(barrier, inc=1, device_id={"kv": to}, device_id_type=MESH)
        return carry

    def greet_tp(step, carry):
        pl.semaphore_signal(
            barrier, inc=1, device_id={"tp": lax.rem(my_tp + step, tps)}, device_id_type=MESH
        )
        return carry

    lax.fori_loop(1, depth, greet_depth, 0, unroll=depth <= 4)
    lax.fori_loop(1, group, greet_plane, 0, unroll=group <= 4)
    lax.fori_loop(1, tps, greet_tp, 0)

    smalls = []
    for at, (src, dst) in enumerate(
        (
            (tokens_hbm, tokens),
            (gain_first_hbm, gain_first),
            (gain_mixer_hbm, gain_mixer),
            (beta_hbm, beta_weight),
            (decay_hbm, decay_weight),
            (rate_hbm, decay_rate),
            (bias_hbm, decay_bias),
            (lengths_hbm, lengths),
            (head_gain_hbm, head_gain),
            (gain_second_hbm, gain_second),
        )
    ):
        small = pltpu.make_async_copy(src, dst, small_sem.at[at])
        small.start()
        smalls.append(small)

    loads = []
    for at, (src, dst) in enumerate(
        (
            (first_gate_hbm, first_gate),
            (first_up_hbm, first_up),
            (first_down_hbm, first_down),
            (query_hbm, query_w),
            (key_hbm, key_w),
            (value_hbm, value_w),
            (outgate_hbm, outgate_w),
            (state_hbm.at[0], state),
            (out_hbm, out_w),
            (second_gate_hbm, second_gate),
            (second_up_hbm, second_up),
            (second_down_hbm, second_down),
        )
    ):
        load = pltpu.make_async_copy(src, dst, load_sem.at[at])
        load.start()
        loads.append(load)

    spread_rows, half = 2 * rows, NEW
    at_row = lax.broadcasted_iota(jnp.int32, (spread_rows, rows), 0)
    at_col = lax.broadcasted_iota(jnp.int32, (spread_rows, rows), 1)
    source = (at_row // (2 * half)) * half + at_row % half
    top = (at_row % (2 * half)) < half
    hit = source == at_col
    spread_top[...] = jnp.where(hit & top, 1.0, 0.0).astype(BF16)
    spread_low[...] = jnp.where(hit & jnp.logical_not(top), 1.0, 0.0).astype(BF16)

    smalls[0].wait()
    own = pl.ds(pl.multiple_of(my_tp * own_rows, own_rows), own_rows)
    arrived[own, :] = tokens[...].astype(F32)
    place_row = lax.broadcasted_iota(jnp.int32, (rows, rows), 0)
    place_col = lax.broadcasted_iota(jnp.int32, (rows, rows), 1)
    block = place_row // half
    wanted = ((block % depth) * group + block // depth) * half + place_row % half
    natural[...] = jnp.where(wanted == place_col, 1.0, 0.0).astype(BF16)
    pl.semaphore_wait(barrier, depth - 1 + group - 1 + tps - 1)

    def all_tp(src, dst, stage, part):
        def one(step, carry):
            pltpu.make_async_remote_copy(
                src_ref=src,
                dst_ref=dst,
                send_sem=pair_sem.at[0, stage],
                recv_sem=pair_sem.at[1, stage],
                device_id={"tp": lax.rem(my_tp + step, tps)},
                device_id_type=MESH,
            ).start()
            return carry

        lax.fori_loop(1, tps, one, 0)

        def settle(sem):
            def one_wait(step, carry):
                pltpu.make_async_copy(part, part, sem).wait()
                return carry

            lax.fori_loop(1, tps, one_wait, 0)

        settle(pair_sem.at[1, stage])
        settle(pair_sem.at[0, stage])

    all_tp(arrived.at[own, :], arrived.at[own, :], 0, arrived.at[pl.ds(0, own_rows), :])
    resid[...] = jnp.dot(
        natural[...], arrived[...].astype(BF16), preferred_element_type=F32
    )

    def spread(matrix_top, matrix_low):
        low = jnp.dot(spread_low[...], matrix_low, preferred_element_type=F32)
        high = jnp.dot(spread_top[...], matrix_top, preferred_element_type=F32)
        return high, low

    def norm_operand(gain):
        whole = resid[...]
        squares = jnp.sum(whole * whole, axis=1, keepdims=True)
        operand = (whole * gain[...]).astype(BF16)
        squares_top = squares.astype(BF16)
        squares_low = (squares - squares_top.astype(F32)).astype(BF16)
        high, low = spread(operand, operand)
        sq_high, sq_low = spread(
            jnp.broadcast_to(squares_top.astype(F32), (rows, LANES)).astype(BF16),
            jnp.broadcast_to(squares_low.astype(F32), (rows, LANES)).astype(BF16),
        )
        return high.astype(BF16), low.astype(BF16), sq_high + sq_low

    def rs_first(bufs, sems, c, start, size, swapped):
        send, mid, _, _, swap_mid, _, _, _, _, _ = bufs
        cols = pl.ds(start, size)
        stage = sems // 6
        if swapped:
            count, place, sem = depth, my_depth, sems + 4
        else:
            count, place, sem = group, my_plane, sems

        def source(to):
            return send.at[:, to, :, cols] if swapped else send.at[to, :, :, cols]

        early = not swapped and c == early_of(bufs[8])
        target = swap_mid.at[place] if swapped else mid.at[place, :, :, cols]
        pltpu.make_async_copy(source(place), target, recv_sem.at[sems, c]).start()

        def one(step, carry):
            to = lax.rem(place + step, count)
            kv = to * group + my_plane if swapped else my_depth * group + to
            pltpu.make_async_remote_copy(
                src_ref=source(to),
                dst_ref=target,
                send_sem=early_sem.at[stage] if early else send_sem.at[sem],
                recv_sem=recv_sem.at[sems, c],
                device_id={"kv": kv},
                device_id_type=MESH,
            ).start()
            return carry

        lax.fori_loop(1, count, one, 0, unroll=count <= 4)

    def early_part(bufs, start, size):
        return bufs[1].at[pl.ds(0, group - 1), :, :, pl.ds(start, size)]

    def rs_begin(bufs, sems, order, sums_at, fill, sizes, header, cut):
        def head(begin, end):
            rs_first(bufs, sems, 0, begin, end - begin, False)

        whole = header + sizes[0]
        first = header + cut
        for at, c in enumerate(order):
            if c:
                fill(c, 0, sizes[c])
                rs_first(bufs, sems, c, *sums_at(c))
            elif not paired:
                fill(0, 0, sizes[0])
                head(0, whole)
            else:
                fill(0, 0, cut)

                @pl.when(jnp.logical_not(late))
                def _():
                    head(0, first)

                if first < whole:
                    fill(0, cut, sizes[0])

                    @pl.when(jnp.logical_not(late))
                    def _():
                        head(first, whole)

            if paired and at == min(1, len(order) - 1):

                @pl.when(late)
                def _():
                    pl.semaphore_wait(turn_sem.at[sems // 6], 1)
                    head(0, whole)

    def hand_over(bufs, sems, start, size):
        part = early_part(bufs, start, size)
        pltpu.make_async_copy(part, part, early_sem.at[sems // 6]).wait()
        if paired:

            @pl.when(jnp.logical_not(late))
            def _():
                pl.semaphore_signal(
                    turn_sem.at[sems // 6], inc=1, device_id={"tp": partner}, device_id_type=MESH
                )

    def rs_second(bufs, sems, c, start, size, swapped):
        _, mid, red, fin, swap_mid, swap_red, swap_fin, _, _, _ = bufs
        if swapped:
            came, kept, last, base = swap_mid, swap_red, swap_fin, 0
            count, place, sem = group, my_plane, sems + 5
        else:
            came, kept, last, base = mid, red, fin, start
            count, place, sem = depth, my_depth, sems + 1
        cols = pl.ds(base, size)
        part = came.at[:, :, :, cols]
        pltpu.make_async_copy(part, part, recv_sem.at[sems, c]).wait()
        for d in range(count):
            for at, wide in chunks_of(size, 512):
                span_at = slice(base + at, base + at + wide)
                value = came[0, d, :, span_at].astype(F32)
                for g in range(1, came.shape[0]):
                    value = value + came[g, d, :, span_at].astype(F32)
                kept[d, :, span_at] = value.astype(BF16)
        pltpu.make_async_copy(
            kept.at[place, :, cols], last.at[place, :, cols], recv_sem.at[sems + 1, c]
        ).start()

        def one(step, carry):
            to = lax.rem(place + step, count)
            kv = my_depth * group + to if swapped else to * group + my_plane
            pltpu.make_async_remote_copy(
                src_ref=kept.at[to, :, cols],
                dst_ref=last.at[place, :, cols],
                send_sem=send_sem.at[sem],
                recv_sem=recv_sem.at[sems + 1, c],
                device_id={"kv": kv},
                device_id_type=MESH,
            ).start()
            return carry

        lax.fori_loop(1, count, one, 0, unroll=count <= 4)

    def rs_wait(bufs, sems, c, start, size, swapped):
        part = bufs[6] if swapped else bufs[3].at[:, :, pl.ds(start, size)]
        pltpu.make_async_copy(part, part, recv_sem.at[sems + 1, c]).wait()

    def ag_depth(bufs, sems, c, start, size):
        buffer = bufs[7]
        mine = buffer.at[my_plane, my_depth, :, pl.ds(start, size)]

        def one(step, carry):
            pltpu.make_async_remote_copy(
                src_ref=mine,
                dst_ref=mine,
                send_sem=send_sem.at[sems + 2],
                recv_sem=recv_sem.at[sems + 2, c],
                device_id={"kv": lax.rem(my_depth + step, depth) * group + my_plane},
                device_id_type=MESH,
            ).start()
            return carry

        lax.fori_loop(1, depth, one, 0, unroll=depth <= 4)

    def ag_direct(bufs, sems, c, start, size):
        buffer = bufs[7]
        mine = buffer.at[my_plane, my_depth, :, pl.ds(start, size)]

        def one(step, carry):
            far, across = step // (group - 1), 1 + lax.rem(step, group - 1)
            to_depth = lax.rem(my_depth + 1 + far, depth)
            to_plane = lax.rem(my_plane + across, group)
            pltpu.make_async_remote_copy(
                src_ref=mine,
                dst_ref=mine,
                send_sem=send_sem.at[sems + 3],
                recv_sem=recv_sem.at[sems + 3, c],
                device_id={"kv": to_depth * group + to_plane},
                device_id_type=MESH,
            ).start()
            return carry

        lax.fori_loop(0, depth * (group - 1), one, 0, unroll=n <= 16)

    def ag_plane(bufs, sems, c, start, size):
        buffer = bufs[7]
        cols = pl.ds(start, size)
        mine = buffer.at[my_plane, :, :, cols]

        def one(step, carry):
            pltpu.make_async_remote_copy(
                src_ref=mine,
                dst_ref=mine,
                send_sem=send_sem.at[sems + 3],
                recv_sem=recv_sem.at[sems + 3, c],
                device_id={"kv": my_depth * group + lax.rem(my_plane + step, group)},
                device_id_type=MESH,
            ).start()
            return carry

        lax.fori_loop(1, group, one, 0, unroll=group <= 4)

    def ag_near(bufs, sems, c, start, size):
        part = bufs[7].at[0, pl.ds(0, depth - 1), :, pl.ds(start, size)]
        pltpu.make_async_copy(part, part, recv_sem.at[sems + 2, c]).wait()

    def ag_wait(bufs, sems, c, start, size):
        part = bufs[7].at[pl.ds(0, group - 1), :, :, pl.ds(start, size)]
        pltpu.make_async_copy(part, part, recv_sem.at[sems + 3, c]).wait()

    def all_sent(bufs, sems):
        send, mid, red, fin, swap_mid, swap_red, swap_fin, buffer, _, width = bufs
        parts = [
            mid.at[pl.ds(0, group - 1), :, :, pl.ds(0, mid.shape[3] - width)],
            fin.at[pl.ds(0, depth - 1)],
            buffer.at[0, pl.ds(0, depth - 1)],
            buffer.at[pl.ds(0, group - 1)],
        ]
        if mid.shape[3] < send.shape[3]:
            parts += [swap_mid.at[pl.ds(0, depth - 1)], swap_fin.at[pl.ds(0, group - 1)]]
        for at, part in enumerate(parts):
            if min(part.shape) > 0:
                pltpu.make_async_copy(part, part, send_sem.at[sems + at]).wait()

    def put(send, start, size, value):
        send[:, :, :, start : start + size] = value.reshape(group, depth, 2 * half, size).astype(
            BF16
        )

    def total(bufs, start, size):
        fin, begin = bufs[3], start
        if start >= fin.shape[2]:
            fin, begin = bufs[6], start - fin.shape[2]
        value = fin[0, :, begin : begin + size].astype(F32)
        for k in range(1, fin.shape[0]):
            value = value + fin[k, :, begin : begin + size].astype(F32)
        return value

    def inverse_rms(bufs):
        squares = total(bufs, 0, LANES)
        return lax.rsqrt((squares[:half] + squares[half:]) / model + EPS)

    def stacked(buffer, start, size):
        flat = buffer[:, :, :, start : start + size].astype(F32).reshape(rows, size)
        return flat.astype(BF16)

    def in_order(count):
        order = list(range(count))
        if swaps(count):
            order = order[: count - 2] + [count - 1, count - 2]
        return [(stage, c) for stage in range(4) for c in order]

    def last_of(count, most):
        return [c for _, c in in_order(count)][:count][max(0, count - most) :]

    def in_issue(count):
        order = list(range(count))
        return order[:1] + order[-1:] + order[1:-1] if swaps(count) else order

    def feed_forward(before, gain, gate, up, down, waits, bufs, pair, sems, tp_sems):
        send, hidden = bufs[0], bufs[7]
        for ready in before:
            ready.wait()
        high, low, squares = norm_operand(gain)
        units = gate.shape[1]
        count = pieces(units // LANES, 4)
        sizes = shares(units, count)
        starts = [sum(sizes[:c]) for c in range(count)]
        put(send, 0, LANES, squares)
        waits[0].wait()
        waits[1].wait()

        def sums_at(c):
            swapped = swaps(count) and c == count - 1
            if c == 0:
                return 0, LANES + sizes[0], False
            return LANES + starts[c], sizes[c], swapped

        def fill(c, begin, end):
            for at, wide in chunks_of(end - begin, 512):
                lo = starts[c] + begin + at
                put(
                    send,
                    LANES + lo,
                    wide,
                    jnp.dot(high, gate[:, lo : lo + wide], preferred_element_type=F32)
                    + jnp.dot(low, up[:, lo : lo + wide], preferred_element_type=F32),
                )

        cut = min(HEAD_CUT * LANES, sizes[0])
        rs_begin(bufs, sems, in_issue(count), sums_at, fill, sizes, LANES, cut)
        hand_over(bufs, sems, *sums_at(early_of(count))[:2])
        branch = jnp.zeros((rows, width), F32)
        slow = last_of(count, HALF_DIRECT[0])
        fast = last_of(count, HALF_DIRECT[1]) if paired else slow

        def where(c, wanted, step, *span):
            on_slow, on_fast = (c in slow) == wanted, (c in fast) == wanted
            if on_slow and on_fast:
                step(bufs, sems, c, *span)
            elif on_slow or on_fast:

                @pl.when(late if on_fast else jnp.logical_not(late))
                def _():
                    step(bufs, sems, c, *span)

        scale, down_ready = None, []
        for stage, c in in_order(count):
            if stage == 0:
                rs_second(bufs, sems, c, *sums_at(c))
            elif stage == 1:
                rs_wait(bufs, sems, c, *sums_at(c))
                if c == 0:
                    scale = inverse_rms(bufs)
                for at, wide in chunks_of(sizes[c], LANES):
                    lo = starts[c] + at
                    both = total(bufs, LANES + lo, wide)
                    hidden[my_plane, my_depth, :, lo : lo + wide] = (
                        silu(both[:half] * scale) * (both[half:] * scale)
                    ).astype(BF16)
                ag_depth(bufs, sems, c, starts[c], sizes[c])
                where(c, True, ag_direct, starts[c], sizes[c])
            elif stage == 2:
                where(c, False, ag_near, starts[c], sizes[c])
                where(c, False, ag_plane, starts[c], sizes[c])
            else:
                where(c, True, ag_near, starts[c], sizes[c])
                ag_wait(bufs, sems, c, starts[c], sizes[c])
                if not down_ready:
                    down_ready.append(waits[2].wait())
                branch = branch + jnp.dot(
                    stacked(hidden, starts[c], sizes[c]),
                    down[starts[c] : starts[c] + sizes[c], :],
                    preferred_element_type=F32,
                )
        pair[my_tp] = branch
        all_tp(pair.at[my_tp], pair.at[my_tp], tp_sems, pair.at[0])
        branch = pair[0]
        for t in range(1, tps):
            branch = branch + pair[t]
        resid[...] = (resid[...] + 0.5 * branch).astype(BF16).astype(F32)

    half_count = pieces(first_gate.shape[1] // LANES, 4)
    half_sizes = shares(first_gate.shape[1], half_count)
    mixer_count = pieces(heads, 4)
    mixer_size = 2 * heads * HEAD_DIM // mixer_count

    def early_width(before, sizes):
        at = early_of(len(sizes))
        return sizes[at] if at else before + sizes[0]

    half_early = (half_count, early_width(LANES, half_sizes))
    mixer_early = (mixer_count, early_width(2 * LANES, [mixer_size] * mixer_count))
    first_bufs = (*first_sums, hidden_first, *half_early)
    mixer_bufs = (*mixer_sums, hidden_mixer, *mixer_early)
    second_bufs = (*second_sums, hidden_second, *half_early)
    send_mixer = mixer_sums[0]
    feed_forward(
        smalls[1:2], gain_first, first_gate, first_up, first_down, loads[0:3],
        first_bufs, pair_first, 0, 1,
    )

    for small in smalls[2:9]:
        small.wait()
    high, low, squares = norm_operand(gain_mixer)
    all_heads = beta_weight.shape[0]
    across = (((1,), (1,)), ((), ()))
    put(send_mixer, 0, LANES, squares)
    send_mixer[:, :, :, LANES : 2 * LANES] = jnp.zeros((group, depth, 2 * half, LANES), BF16)
    small = lax.dot_general(
        high, beta_weight[...], across, preferred_element_type=F32
    ) + lax.dot_general(low, decay_weight[...], across, preferred_element_type=F32)
    put(send_mixer, LANES, all_heads, small)
    for load in loads[3:7]:
        load.wait()
    count = pieces(heads, 4)
    batch = heads // count
    size = batch * HEAD_DIM

    def mixed_at(c):
        start = 2 * LANES + 2 * c * size
        swapped = swaps(count) and c == count - 1
        return (0, 2 * LANES + 2 * size, False) if c == 0 else (start, 2 * size, swapped)

    def fill(c, begin, end):
        for at, (first, second) in enumerate(((query_w, value_w), (key_w, outgate_w))):
            if not begin <= at * size < end:
                continue
            lo = c * size
            put(
                send_mixer,
                2 * LANES + (2 * c + at) * size,
                size,
                jnp.dot(high, first[:, lo : lo + size], preferred_element_type=F32)
                + jnp.dot(low, second[:, lo : lo + size], preferred_element_type=F32),
            )

    rs_begin(
        mixer_bufs, 6, in_issue(count), mixed_at, fill, [2 * size] * count, 2 * LANES, size
    )
    hand_over(mixer_bufs, 6, *mixed_at(early_of(count))[:2])
    lane = lax.broadcasted_iota(jnp.int32, (half, LANES), 1)
    slot = lax.broadcasted_iota(jnp.int32, (half, LANES), 0)
    live = jnp.where(slot < lengths[0], 1.0, 0.0)
    loads[7].wait()
    for h in range(heads):
        old = state[h]
        top = old.astype(BF16)
        split[h, :, :HEAD_DIM] = top
        split[h, :, HEAD_DIM:] = (old - top.astype(F32)).astype(BF16)
    for stage, c in in_order(count)[:count]:
        rs_second(mixer_bufs, 6, c, *mixed_at(c))
    groups = [range(c, min(c + 2, count)) for c in range(0, count, 2)]
    scale, logits, grown = None, None, []
    for group_of in groups:
        for c in group_of:
            rs_wait(mixer_bufs, 6, c, *mixed_at(c))
        if scale is None:
            scale = inverse_rms(mixer_bufs)
            logits = total(mixer_bufs, LANES, LANES)
        for h in range(group_of[0] * batch, (group_of[-1] + 1) * batch):
            c = h // batch
            base = 2 * LANES + 2 * c * size + (h - c * batch) * HEAD_DIM
            both = total(mixer_bufs, base, HEAD_DIM)
            query, value = silu(both[:half] * scale), silu(both[half:] * scale)
            both = total(mixer_bufs, base + size, HEAD_DIM)
            keyvec, outgate = silu(both[:half] * scale), silu(both[half:] * scale)
            query = query * lax.rsqrt(jnp.sum(query * query, axis=1, keepdims=True) + EPS)
            query = query * HEAD_DIM ** (-0.5)
            keyvec = keyvec * lax.rsqrt(jnp.sum(keyvec * keyvec, axis=1, keepdims=True) + EPS)
            mine = lane == my_tp * heads + h
            beta_logit = jnp.sum(jnp.where(mine, logits[:half] * scale, 0.0), axis=1, keepdims=True)
            decay_logit = jnp.sum(jnp.where(mine, logits[half:] * scale, 0.0), axis=1, keepdims=True)
            beta_logit = jnp.broadcast_to(beta_logit, (half, LANES))
            decay_logit = jnp.broadcast_to(decay_logit, (half, LANES)) + decay_bias[0, h]
            beta = live / (1.0 + jnp.exp(-beta_logit))
            soft = jnp.maximum(decay_logit, 0.0) + jnp.log(1.0 + jnp.exp(-jnp.abs(decay_logit)))
            decay = -decay_rate[0, h] * soft * live
            reach = jnp.zeros_like(decay)
            for i in range(NEW):
                reach = reach + jnp.where(slot >= i, decay[i : i + 1], 0.0)
            before = jnp.exp(reach)
            asked = jnp.concatenate([keyvec, query], axis=0)
            top = asked.astype(BF16).astype(F32)
            found = jnp.dot(
                jnp.concatenate([top, asked - top], axis=0).astype(BF16),
                split[h],
                preferred_element_type=F32,
            )
            held = (
                found[: 2 * half, :HEAD_DIM]
                + found[2 * half :, :HEAD_DIM]
                + found[: 2 * half, HEAD_DIM:]
            )
            update = beta * (value - before * held[:half])
            output = before * held[half:]
            for i in range(NEW):
                between = jnp.where(slot >= i, jnp.exp(jnp.minimum(reach - reach[i : i + 1], 0.0)), 0.0)
                row = keyvec[i : i + 1]
                alike = jnp.sum(keyvec * row, axis=1, keepdims=True)
                fixed = update[i : i + 1]
                update = update - jnp.where(slot > i, beta * between * alike * fixed, 0.0)
                output = output + between * jnp.sum(query * row, axis=1, keepdims=True) * fixed
            last = reach[NEW - 1 : NEW]
            grown.append((keyvec, update * jnp.exp(last - reach), jnp.exp(last)))
            output = output * live
            output = output * lax.rsqrt(jnp.mean(output * output, axis=1, keepdims=True) + EPS)
            output = output * head_gain[...] * outgate
            hidden_mixer[my_plane, my_depth, :, h * HEAD_DIM : (h + 1) * HEAD_DIM] = output.astype(
                BF16
            )
        part = (group_of[0], group_of[0] * size, len(group_of) * size)
        ag_depth(mixer_bufs, 6, *part)
        ag_direct(mixer_bufs, 6, *part)
    for h, (keyvec, gained, kept) in enumerate(grown):
        zero = jnp.zeros_like(keyvec)
        new_state[0, h] = state[h] * kept + lax.dot_general(
            jnp.concatenate([keyvec, zero], axis=0),
            jnp.concatenate([gained, zero], axis=0),
            (((0,), (0,)), ((), ())),
            precision=lax.Precision.HIGHEST,
            preferred_element_type=F32,
        )
    loads[8].wait()
    branch = jnp.zeros((rows, width), F32)
    for group_of in groups:
        start, wide = group_of[0] * size, len(group_of) * size
        ag_near(mixer_bufs, 6, group_of[0], start, wide)
        ag_wait(mixer_bufs, 6, group_of[0], start, wide)
        branch = branch + jnp.dot(
            stacked(hidden_mixer, start, wide),
            out_w[start : start + wide, :],
            preferred_element_type=F32,
        )
    pair_mixer[my_tp] = branch
    all_tp(pair_mixer.at[my_tp], pair_mixer.at[my_tp], 2, pair_mixer.at[0])
    branch = pair_mixer[0]
    for t in range(1, tps):
        branch = branch + pair_mixer[t]
    resid[...] = (resid[...] + branch).astype(BF16).astype(F32)

    feed_forward(
        smalls[9:10], gain_second, second_gate, second_up, second_down, loads[9:12],
        second_bufs, pair_second, 12, 3,
    )
    arrived[...] = lax.dot_general(
        natural[...], resid[...].astype(BF16), (((0,), (0,)), ((), ())), preferred_element_type=F32
    )
    layer_out[...] = arrived[own, :].astype(BF16)
    all_sent(first_bufs, 0)
    all_sent(mixer_bufs, 6)
    all_sent(second_bufs, 12)


def solution(mesh):
    n, tps = mesh.shape["kv"], mesh.shape["tp"]

    def on_device(
        tokens,
        lengths,
        memory_state,
        gain_first,
        first_gate,
        first_up,
        first_down,
        gain_mixer,
        query_weight,
        key_weight,
        value_weight,
        outgate_weight,
        beta_weight,
        decay_weight,
        decay_rate,
        decay_bias,
        head_gain,
        out_weight,
        gain_second,
        second_gate,
        second_up,
        second_down,
    ):
        rows = tokens.shape[0] * tps
        width = tokens.shape[1]
        units = first_gate.shape[1]
        span = query_weight.shape[1]
        group = pieces(n, 4)
        depth = n // group
        half_parts = pieces(units // LANES, 4)
        mixer_parts = pieces(memory_state.shape[1], 4)
        vmem = pl.BlockSpec(memory_space=pltpu.VMEM)
        hbm = pl.BlockSpec(memory_space=pltpu.HBM)

        def like(array):
            return pltpu.VMEM(array.shape, array.dtype)

        def owners(before, sizes):
            swapped = swaps(len(sizes))
            last = sizes[-1] if swapped else LANES
            columns = before + sum(sizes)
            kept = columns - (last if swapped else 0)
            return (
                pltpu.VMEM((group, depth, 2 * NEW, columns), BF16),
                pltpu.VMEM((group, depth, 2 * NEW, kept), BF16),
                pltpu.VMEM((depth, 2 * NEW, kept), BF16),
                pltpu.VMEM((depth, 2 * NEW, kept), BF16),
                pltpu.VMEM((depth, group, 2 * NEW, last), BF16),
                pltpu.VMEM((group, 2 * NEW, last), BF16),
                pltpu.VMEM((group, 2 * NEW, last), BF16),
            )

        def gathered(columns):
            return pltpu.VMEM((group, depth, NEW, columns), BF16)

        def pairs():
            return pltpu.VMEM((tps, rows, width), F32)

        parts = pl.pallas_call(
            functools.partial(layer_kernel, n, tps),
            name="layer",
            out_shape=(
                pltpu.VMEM(tokens.shape, BF16),
                pltpu.VMEM(memory_state.shape, F32),
            ),
            in_specs=[hbm] * 22,
            out_specs=(vmem, vmem),
            scratch_shapes=[
                like(tokens),
                pltpu.SMEM(lengths.shape, lengths.dtype),
                pltpu.VMEM((1, width), F32),
                pltpu.VMEM((1, width), F32),
                pltpu.VMEM(beta_weight.shape[::-1], BF16),
                pltpu.VMEM(decay_weight.shape[::-1], BF16),
                pltpu.SMEM((1, decay_rate.shape[0]), F32),
                pltpu.SMEM((1, decay_bias.shape[0]), F32),
                pltpu.VMEM((1, HEAD_DIM), F32),
                pltpu.VMEM((1, width), F32),
                like(first_gate),
                like(first_up),
                like(first_down),
                like(query_weight),
                like(key_weight),
                like(value_weight),
                like(outgate_weight),
                like(out_weight),
                like(second_gate),
                like(second_up),
                like(second_down),
                pltpu.VMEM(memory_state.shape[1:], F32),
                pltpu.VMEM((*memory_state.shape[1:3], 2 * HEAD_DIM), BF16),
                pltpu.VMEM((rows, width), F32),
                pltpu.VMEM((2 * rows, rows), BF16),
                pltpu.VMEM((2 * rows, rows), BF16),
                pltpu.VMEM((rows, width), F32),
                pltpu.VMEM((rows, rows), BF16),
                owners(LANES, shares(units, half_parts)),
                owners(2 * LANES, [2 * span // mixer_parts] * mixer_parts),
                owners(LANES, shares(units, half_parts)),
                gathered(units),
                gathered(span),
                gathered(units),
                pairs(),
                pairs(),
                pairs(),
                pltpu.SemaphoreType.DMA((12,)),
                pltpu.SemaphoreType.DMA((18,)),
                pltpu.SemaphoreType.DMA((18, 4)),
                pltpu.SemaphoreType.DMA((2, 4)),
                pltpu.SemaphoreType.DMA((3,)),
                pltpu.SemaphoreType.REGULAR((3,)),
                pltpu.SemaphoreType.DMA((10,)),
            ],
            compiler_params=pltpu.CompilerParams(
                collective_id=0,
                has_side_effects=True,
                vmem_limit_bytes=60 * 1024 * 1024,
            ),
        )(
            tokens,
            lengths,
            memory_state,
            gain_first.reshape(1, -1),
            first_gate,
            first_up,
            first_down,
            gain_mixer.reshape(1, -1),
            query_weight,
            key_weight,
            value_weight,
            outgate_weight,
            beta_weight.T,
            decay_weight.T,
            decay_rate.reshape(1, -1),
            decay_bias.reshape(1, -1),
            head_gain.reshape(1, -1),
            out_weight,
            gain_second.reshape(1, -1),
            second_gate,
            second_up,
            second_down,
        )
        return pl.pallas_call(
            put_out,
            name="put_out",
            out_shape=(
                jax.ShapeDtypeStruct(tokens.shape, BF16),
                jax.ShapeDtypeStruct(memory_state.shape, F32),
            ),
            in_specs=[vmem, vmem],
            out_specs=(hbm, hbm),
            scratch_shapes=[pltpu.SemaphoreType.DMA((2,))],
            compiler_params=pltpu.CompilerParams(vmem_limit_bytes=2 * 1024 * 1024),
        )(*parts)

    in_specs = (
        P("tp", "kv"),
        P("kv"),
        P("kv", "tp", None, None),
        P("kv"),
        P("kv", "tp"),
        P("kv", "tp"),
        P("tp", "kv"),
        P("kv"),
        P("kv", "tp"),
        P("kv", "tp"),
        P("kv", "tp"),
        P("kv", "tp"),
        P("kv", None),
        P("kv", None),
        P("tp"),
        P("tp"),
        P(),
        P("tp", "kv"),
        P("kv"),
        P("kv", "tp"),
        P("kv", "tp"),
        P("tp", "kv"),
    )
    out_specs = (P("tp", "kv"), P("kv", "tp", None, None))
    return jax.shard_map(
        on_device, mesh=mesh, in_specs=in_specs, out_specs=out_specs, check_vma=False
    )
```

```python
import functools

import jax
import jax.numpy as jnp
from jax import lax
from jax.experimental import pallas as pl
from jax.experimental.pallas import tpu as pltpu
from jax.sharding import PartitionSpec as P

MESH = pl.DeviceIdType.MESH
HEAD_DIM = 128
LANES = 128
NEW = 4
EPS = 1e-06
SHIFT = ((0, -1), (1, -1), (2, 2))
HEAD_CUT = 2
EARLY = 1
HALF_DIRECT = (2, 1)
F32 = jnp.float32
BF16 = jnp.bfloat16


def silu(x):
    return x / (1.0 + jnp.exp(-x))


def pieces(total, most):
    return next(k for k in range(most, 0, -1) if total % k == 0)


def swaps(count):
    return count > 2


def shares(units, count):
    tiles = units // LANES // count
    if swaps(count) and tiles > 3:
        parts = [tiles] * count
        for c, more in SHIFT:
            parts[c] += more
    else:
        parts = [tiles] * count
    return [part * LANES for part in parts]


def early_of(count):
    return min(EARLY, count - 1 - int(swaps(count)))


def chunks_of(total, step):
    return [(c, min(step, total - c)) for c in range(0, total, step)]


def put_out(layer, state, layer_hbm, state_hbm, sem):
    moves = [
        pltpu.make_async_copy(src, dst, sem.at[at])
        for at, (src, dst) in enumerate(((layer, layer_hbm), (state, state_hbm)))
    ]
    for move in moves:
        move.start()
    for move in moves:
        move.wait()


def layer_kernel(
    n,
    tps,
    tokens_hbm,
    lengths_hbm,
    state_hbm,
    gain_first_hbm,
    first_gate_hbm,
    first_up_hbm,
    first_down_hbm,
    gain_mixer_hbm,
    query_hbm,
    key_hbm,
    value_hbm,
    outgate_hbm,
    beta_hbm,
    decay_hbm,
    rate_hbm,
    bias_hbm,
    head_gain_hbm,
    out_hbm,
    gain_second_hbm,
    second_gate_hbm,
    second_up_hbm,
    second_down_hbm,
    layer_out,
    new_state,
    tokens,
    lengths,
    gain_first,
    gain_mixer,
    beta_weight,
    decay_weight,
    decay_rate,
    decay_bias,
    head_gain,
    gain_second,
    first_gate,
    first_up,
    first_down,
    query_w,
    key_w,
    value_w,
    outgate_w,
    out_w,
    second_gate,
    second_up,
    second_down,
    state,
    split,
    resid,
    spread_top,
    spread_low,
    arrived,
    natural,
    first_sums,
    mixer_sums,
    second_sums,
    hidden_first,
    hidden_mixer,
    hidden_second,
    pair_first,
    pair_mixer,
    pair_second,
    load_sem,
    send_sem,
    recv_sem,
    pair_sem,
    early_sem,
    turn_sem,
    small_sem,
):
    me = lax.axis_index("kv")
    my_tp = lax.axis_index("tp")
    rows, width = resid.shape
    own_rows = rows // tps
    group = hidden_first.shape[0]
    depth = n // group
    my_plane, my_depth = lax.rem(me, group), me // group
    heads = state.shape[0]
    model = n * width
    paired = tps % 2 == 0
    late = lax.rem(my_tp, 2) == 1
    partner = my_tp + 1 - 2 * lax.rem(my_tp, 2)

    barrier = pltpu.get_barrier_semaphore()

    def greet_plane(step, carry):
        to = my_depth * group + lax.rem(my_plane + step, group)
        pl.semaphore_signal(barrier, inc=1, device_id={"kv": to}, device_id_type=MESH)
        return carry

    def greet_depth(step, carry):
        to = lax.rem(my_depth + step, depth) * group + my_plane
        pl.semaphore_signal(barrier, inc=1, device_id={"kv": to}, device_id_type=MESH)
        return carry

    def greet_tp(step, carry):
        pl.semaphore_signal(
            barrier, inc=1, device_id={"tp": lax.rem(my_tp + step, tps)}, device_id_type=MESH
        )
        return carry

    lax.fori_loop(1, depth, greet_depth, 0, unroll=depth <= 4)
    lax.fori_loop(1, group, greet_plane, 0, unroll=group <= 4)
    lax.fori_loop(1, tps, greet_tp, 0)

    smalls = []
    for at, (src, dst) in enumerate(
        (
            (tokens_hbm, tokens),
            (gain_first_hbm, gain_first),
            (gain_mixer_hbm, gain_mixer),
            (beta_hbm, beta_weight),
            (decay_hbm, decay_weight),
            (rate_hbm, decay_rate),
            (bias_hbm, decay_bias),
            (lengths_hbm, lengths),
            (head_gain_hbm, head_gain),
            (gain_second_hbm, gain_second),
        )
    ):
        small = pltpu.make_async_copy(src, dst, small_sem.at[at])
        small.start()
        smalls.append(small)

    loads = []
    for at, (src, dst) in enumerate(
        (
            (first_gate_hbm, first_gate),
            (first_up_hbm, first_up),
            (first_down_hbm, first_down),
            (query_hbm, query_w),
            (key_hbm, key_w),
            (value_hbm, value_w),
            (outgate_hbm, outgate_w),
            (state_hbm.at[0], state),
            (out_hbm, out_w),
            (second_gate_hbm, second_gate),
            (second_up_hbm, second_up),
            (second_down_hbm, second_down),
        )
    ):
        load = pltpu.make_async_copy(src, dst, load_sem.at[at])
        load.start()
        loads.append(load)

    spread_rows, half = 2 * rows, NEW
    at_row = lax.broadcasted_iota(jnp.int32, (spread_rows, rows), 0)
    at_col = lax.broadcasted_iota(jnp.int32, (spread_rows, rows), 1)
    source = (at_row // (2 * half)) * half + at_row % half
    top = (at_row % (2 * half)) < half
    hit = source == at_col
    spread_top[...] = jnp.where(hit & top, 1.0, 0.0).astype(BF16)
    spread_low[...] = jnp.where(hit & jnp.logical_not(top), 1.0, 0.0).astype(BF16)

    mixer_sums[0][:, :, :, LANES : 2 * LANES] = jnp.zeros((group, depth, 2 * half, LANES), BF16)
    smalls[0].wait()
    own = pl.ds(pl.multiple_of(my_tp * own_rows, own_rows), own_rows)
    arrived[own, :] = tokens[...].astype(F32)
    place_row = lax.broadcasted_iota(jnp.int32, (rows, rows), 0)
    place_col = lax.broadcasted_iota(jnp.int32, (rows, rows), 1)
    block = place_row // half
    wanted = ((block % depth) * group + block // depth) * half + place_row % half
    natural[...] = jnp.where(wanted == place_col, 1.0, 0.0).astype(BF16)
    pl.semaphore_wait(barrier, depth - 1 + group - 1 + tps - 1)

    def all_tp(src, dst, stage, part):
        def one(step, carry):
            pltpu.make_async_remote_copy(
                src_ref=src,
                dst_ref=dst,
                send_sem=pair_sem.at[0, stage],
                recv_sem=pair_sem.at[1, stage],
                device_id={"tp": lax.rem(my_tp + step, tps)},
                device_id_type=MESH,
            ).start()
            return carry

        lax.fori_loop(1, tps, one, 0)

        def settle(sem):
            def one_wait(step, carry):
                pltpu.make_async_copy(part, part, sem).wait()
                return carry

            lax.fori_loop(1, tps, one_wait, 0)

        settle(pair_sem.at[1, stage])
        settle(pair_sem.at[0, stage])

    all_tp(arrived.at[own, :], arrived.at[own, :], 0, arrived.at[pl.ds(0, own_rows), :])
    resid[...] = jnp.dot(
        natural[...], arrived[...].astype(BF16), preferred_element_type=F32
    )

    def spread(matrix_top, matrix_low):
        low = jnp.dot(spread_low[...], matrix_low, preferred_element_type=F32)
        high = jnp.dot(spread_top[...], matrix_top, preferred_element_type=F32)
        return high, low

    def norm_operand(gain):
        whole = resid[...]
        squares = jnp.sum(whole * whole, axis=1, keepdims=True)
        operand = (whole * gain[...]).astype(BF16)
        squares_top = squares.astype(BF16)
        squares_low = (squares - squares_top.astype(F32)).astype(BF16)
        high, low = spread(operand, operand)
        sq_high, sq_low = spread(
            jnp.broadcast_to(squares_top.astype(F32), (rows, LANES)).astype(BF16),
            jnp.broadcast_to(squares_low.astype(F32), (rows, LANES)).astype(BF16),
        )
        return high.astype(BF16), low.astype(BF16), sq_high + sq_low

    def rs_first(bufs, sems, c, start, size, swapped):
        send, mid, _, _, swap_mid, _, _, _, _, _ = bufs
        cols = pl.ds(start, size)
        stage = sems // 6
        if swapped:
            count, place, sem = depth, my_depth, sems + 4
        else:
            count, place, sem = group, my_plane, sems

        def source(to):
            return send.at[:, to, :, cols] if swapped else send.at[to, :, :, cols]

        early = not swapped and c == early_of(bufs[8])
        target = swap_mid.at[place] if swapped else mid.at[place, :, :, cols]
        pltpu.make_async_copy(source(place), target, recv_sem.at[sems, c]).start()

        def one(step, carry):
            to = lax.rem(place + step, count)
            kv = to * group + my_plane if swapped else my_depth * group + to
            pltpu.make_async_remote_copy(
                src_ref=source(to),
                dst_ref=target,
                send_sem=early_sem.at[stage] if early else send_sem.at[sem],
                recv_sem=recv_sem.at[sems, c],
                device_id={"kv": kv},
                device_id_type=MESH,
            ).start()
            return carry

        lax.fori_loop(1, count, one, 0, unroll=count <= 4)

    def early_part(bufs, start, size):
        return bufs[1].at[pl.ds(0, group - 1), :, :, pl.ds(start, size)]

    def rs_begin(bufs, sems, order, sums_at, fill, sizes, header, cut, put_header=None):
        def head(begin, end):
            rs_first(bufs, sems, 0, begin, end - begin, False)

        whole = header + sizes[0]
        first = header + cut
        for at, c in enumerate(order):
            if c:
                fill(c, 0, sizes[c])
                rs_first(bufs, sems, c, *sums_at(c))
            elif not paired:
                if put_header:
                    put_header()
                fill(0, 0, sizes[0])
                head(0, whole)
            else:
                fill(0, 0, cut)

                @pl.when(jnp.logical_not(late))
                def _():
                    head(header if put_header else 0, first)

                if put_header:
                    put_header()

                    @pl.when(jnp.logical_not(late))
                    def _():
                        head(0, header)

                if first < whole:
                    fill(0, cut, sizes[0])

                    @pl.when(jnp.logical_not(late))
                    def _():
                        head(first, whole)

            if paired and at == min(1, len(order) - 1):

                @pl.when(late)
                def _():
                    pl.semaphore_wait(turn_sem.at[sems // 6], 1)
                    head(0, whole)

    def hand_over(bufs, sems, start, size):
        part = early_part(bufs, start, size)
        pltpu.make_async_copy(part, part, early_sem.at[sems // 6]).wait()
        if paired:

            @pl.when(jnp.logical_not(late))
            def _():
                pl.semaphore_signal(
                    turn_sem.at[sems // 6], inc=1, device_id={"tp": partner}, device_id_type=MESH
                )

    def rs_second(bufs, sems, c, start, size, swapped):
        _, mid, red, fin, swap_mid, swap_red, swap_fin, _, _, _ = bufs
        if swapped:
            came, kept, last, base = swap_mid, swap_red, swap_fin, 0
            count, place, sem = group, my_plane, sems + 5
        else:
            came, kept, last, base = mid, red, fin, start
            count, place, sem = depth, my_depth, sems + 1
        cols = pl.ds(base, size)
        part = came.at[:, :, :, cols]
        pltpu.make_async_copy(part, part, recv_sem.at[sems, c]).wait()
        for d in range(count):
            for at, wide in chunks_of(size, 512):
                span_at = slice(base + at, base + at + wide)
                value = came[0, d, :, span_at].astype(F32)
                for g in range(1, came.shape[0]):
                    value = value + came[g, d, :, span_at].astype(F32)
                kept[d, :, span_at] = value.astype(BF16)
        pltpu.make_async_copy(
            kept.at[place, :, cols], last.at[place, :, cols], recv_sem.at[sems + 1, c]
        ).start()

        def one(step, carry):
            to = lax.rem(place + step, count)
            kv = my_depth * group + to if swapped else to * group + my_plane
            pltpu.make_async_remote_copy(
                src_ref=kept.at[to, :, cols],
                dst_ref=last.at[place, :, cols],
                send_sem=send_sem.at[sem],
                recv_sem=recv_sem.at[sems + 1, c],
                device_id={"kv": kv},
                device_id_type=MESH,
            ).start()
            return carry

        lax.fori_loop(1, count, one, 0, unroll=count <= 4)

    def rs_wait(bufs, sems, c, start, size, swapped):
        part = bufs[6] if swapped else bufs[3].at[:, :, pl.ds(start, size)]
        pltpu.make_async_copy(part, part, recv_sem.at[sems + 1, c]).wait()

    def ag_depth(bufs, sems, c, start, size):
        buffer = bufs[7]
        mine = buffer.at[my_plane, my_depth, :, pl.ds(start, size)]

        def one(step, carry):
            pltpu.make_async_remote_copy(
                src_ref=mine,
                dst_ref=mine,
                send_sem=send_sem.at[sems + 2],
                recv_sem=recv_sem.at[sems + 2, c],
                device_id={"kv": lax.rem(my_depth + step, depth) * group + my_plane},
                device_id_type=MESH,
            ).start()
            return carry

        lax.fori_loop(1, depth, one, 0, unroll=depth <= 4)

    def ag_direct(bufs, sems, c, start, size):
        buffer = bufs[7]
        mine = buffer.at[my_plane, my_depth, :, pl.ds(start, size)]

        def one(step, carry):
            far, across = step // (group - 1), 1 + lax.rem(step, group - 1)
            to_depth = lax.rem(my_depth + 1 + far, depth)
            to_plane = lax.rem(my_plane + across, group)
            pltpu.make_async_remote_copy(
                src_ref=mine,
                dst_ref=mine,
                send_sem=send_sem.at[sems + 3],
                recv_sem=recv_sem.at[sems + 3, c],
                device_id={"kv": to_depth * group + to_plane},
                device_id_type=MESH,
            ).start()
            return carry

        lax.fori_loop(0, depth * (group - 1), one, 0, unroll=n <= 16)

    def ag_plane(bufs, sems, c, start, size):
        buffer = bufs[7]
        cols = pl.ds(start, size)
        mine = buffer.at[my_plane, :, :, cols]

        def one(step, carry):
            pltpu.make_async_remote_copy(
                src_ref=mine,
                dst_ref=mine,
                send_sem=send_sem.at[sems + 3],
                recv_sem=recv_sem.at[sems + 3, c],
                device_id={"kv": my_depth * group + lax.rem(my_plane + step, group)},
                device_id_type=MESH,
            ).start()
            return carry

        lax.fori_loop(1, group, one, 0, unroll=group <= 4)

    def ag_near(bufs, sems, c, start, size):
        part = bufs[7].at[0, pl.ds(0, depth - 1), :, pl.ds(start, size)]
        pltpu.make_async_copy(part, part, recv_sem.at[sems + 2, c]).wait()

    def ag_wait(bufs, sems, c, start, size):
        part = bufs[7].at[pl.ds(0, group - 1), :, :, pl.ds(start, size)]
        pltpu.make_async_copy(part, part, recv_sem.at[sems + 3, c]).wait()

    def all_sent(bufs, sems):
        send, mid, red, fin, swap_mid, swap_red, swap_fin, buffer, _, width = bufs
        parts = [
            mid.at[pl.ds(0, group - 1), :, :, pl.ds(0, mid.shape[3] - width)],
            fin.at[pl.ds(0, depth - 1)],
            buffer.at[0, pl.ds(0, depth - 1)],
            buffer.at[pl.ds(0, group - 1)],
        ]
        if mid.shape[3] < send.shape[3]:
            parts += [swap_mid.at[pl.ds(0, depth - 1)], swap_fin.at[pl.ds(0, group - 1)]]
        for at, part in enumerate(parts):
            if min(part.shape) > 0:
                pltpu.make_async_copy(part, part, send_sem.at[sems + at]).wait()

    def put(send, start, size, value):
        send[:, :, :, start : start + size] = value.reshape(group, depth, 2 * half, size).astype(
            BF16
        )

    def total(bufs, start, size):
        fin, begin = bufs[3], start
        if start >= fin.shape[2]:
            fin, begin = bufs[6], start - fin.shape[2]
        value = fin[0, :, begin : begin + size].astype(F32)
        for k in range(1, fin.shape[0]):
            value = value + fin[k, :, begin : begin + size].astype(F32)
        return value

    def inverse_rms(bufs):
        squares = total(bufs, 0, LANES)
        return lax.rsqrt((squares[:half] + squares[half:]) / model + EPS)

    def stacked(buffer, start, size):
        flat = buffer[:, :, :, start : start + size].astype(F32).reshape(rows, size)
        return flat.astype(BF16)

    def in_order(count):
        order = list(range(count))
        if swaps(count):
            order = order[: count - 2] + [count - 1, count - 2]
        return [(stage, c) for stage in range(4) for c in order]

    def last_of(count, most):
        return [c for _, c in in_order(count)][:count][max(0, count - most) :]

    def in_issue(count):
        order = list(range(count))
        return order[:1] + order[-1:] + order[1:-1] if swaps(count) else order

    def feed_forward(before, gain, gate, up, down, waits, bufs, pair, sems, tp_sems):
        send, hidden = bufs[0], bufs[7]
        for ready in before:
            ready.wait()
        high, low, squares = norm_operand(gain)
        units = gate.shape[1]
        count = pieces(units // LANES, 4)
        sizes = shares(units, count)
        starts = [sum(sizes[:c]) for c in range(count)]
        put(send, 0, LANES, squares)
        waits[0].wait()
        waits[1].wait()

        def sums_at(c):
            swapped = swaps(count) and c == count - 1
            if c == 0:
                return 0, LANES + sizes[0], False
            return LANES + starts[c], sizes[c], swapped

        def fill(c, begin, end):
            for at, wide in chunks_of(end - begin, 512):
                lo = starts[c] + begin + at
                put(
                    send,
                    LANES + lo,
                    wide,
                    jnp.dot(high, gate[:, lo : lo + wide], preferred_element_type=F32)
                    + jnp.dot(low, up[:, lo : lo + wide], preferred_element_type=F32),
                )

        cut = min(HEAD_CUT * LANES, sizes[0])
        rs_begin(bufs, sems, in_issue(count), sums_at, fill, sizes, LANES, cut)
        hand_over(bufs, sems, *sums_at(early_of(count))[:2])
        branch = jnp.zeros((rows, width), F32)
        slow = last_of(count, HALF_DIRECT[0])
        fast = last_of(count, HALF_DIRECT[1]) if paired else slow

        def where(c, wanted, step, *span):
            on_slow, on_fast = (c in slow) == wanted, (c in fast) == wanted
            if on_slow and on_fast:
                step(bufs, sems, c, *span)
            elif on_slow or on_fast:

                @pl.when(late if on_fast else jnp.logical_not(late))
                def _():
                    step(bufs, sems, c, *span)

        scale, down_ready = None, []
        for stage, c in in_order(count):
            if stage == 0:
                rs_second(bufs, sems, c, *sums_at(c))
            elif stage == 1:
                rs_wait(bufs, sems, c, *sums_at(c))
                if c == 0:
                    scale = inverse_rms(bufs)
                for at, wide in chunks_of(sizes[c], LANES):
                    lo = starts[c] + at
                    both = total(bufs, LANES + lo, wide)
                    hidden[my_plane, my_depth, :, lo : lo + wide] = (
                        silu(both[:half] * scale) * (both[half:] * scale)
                    ).astype(BF16)
                ag_depth(bufs, sems, c, starts[c], sizes[c])
                where(c, True, ag_direct, starts[c], sizes[c])
            elif stage == 2:
                where(c, False, ag_near, starts[c], sizes[c])
                where(c, False, ag_plane, starts[c], sizes[c])
            else:
                where(c, True, ag_near, starts[c], sizes[c])
                ag_wait(bufs, sems, c, starts[c], sizes[c])
                if not down_ready:
                    down_ready.append(waits[2].wait())
                branch = branch + jnp.dot(
                    stacked(hidden, starts[c], sizes[c]),
                    down[starts[c] : starts[c] + sizes[c], :],
                    preferred_element_type=F32,
                )
        pair[my_tp] = branch
        all_tp(pair.at[my_tp], pair.at[my_tp], tp_sems, pair.at[0])
        branch = pair[0]
        for t in range(1, tps):
            branch = branch + pair[t]
        resid[...] = (resid[...] + 0.5 * branch).astype(BF16).astype(F32)

    half_count = pieces(first_gate.shape[1] // LANES, 4)
    half_sizes = shares(first_gate.shape[1], half_count)
    mixer_count = pieces(heads, 4)
    mixer_size = 2 * heads * HEAD_DIM // mixer_count

    def early_width(before, sizes):
        at = early_of(len(sizes))
        return sizes[at] if at else before + sizes[0]

    half_early = (half_count, early_width(LANES, half_sizes))
    mixer_early = (mixer_count, early_width(2 * LANES, [mixer_size] * mixer_count))
    first_bufs = (*first_sums, hidden_first, *half_early)
    mixer_bufs = (*mixer_sums, hidden_mixer, *mixer_early)
    second_bufs = (*second_sums, hidden_second, *half_early)
    send_mixer = mixer_sums[0]
    feed_forward(
        smalls[1:2], gain_first, first_gate, first_up, first_down, loads[0:3],
        first_bufs, pair_first, 0, 1,
    )

    for small in smalls[2:9]:
        small.wait()
    high, low, squares = norm_operand(gain_mixer)
    all_heads = beta_weight.shape[0]
    across = (((1,), (1,)), ((), ()))

    def put_header():
        small = lax.dot_general(
            high, beta_weight[...], across, preferred_element_type=F32
        ) + lax.dot_general(low, decay_weight[...], across, preferred_element_type=F32)
        put(send_mixer, 0, LANES, squares)
        put(send_mixer, LANES, all_heads, small)

    for load in loads[3:7]:
        load.wait()
    count = pieces(heads, 4)
    batch = heads // count
    size = batch * HEAD_DIM

    def mixed_at(c):
        start = 2 * LANES + 2 * c * size
        swapped = swaps(count) and c == count - 1
        return (0, 2 * LANES + 2 * size, False) if c == 0 else (start, 2 * size, swapped)

    def fill(c, begin, end):
        for at, (first, second) in enumerate(((query_w, value_w), (key_w, outgate_w))):
            if not begin <= at * size < end:
                continue
            lo = c * size
            put(
                send_mixer,
                2 * LANES + (2 * c + at) * size,
                size,
                jnp.dot(high, first[:, lo : lo + size], preferred_element_type=F32)
                + jnp.dot(low, second[:, lo : lo + size], preferred_element_type=F32),
            )

    rs_begin(
        mixer_bufs, 6, in_issue(count), mixed_at, fill, [2 * size] * count, 2 * LANES, size,
        put_header,
    )
    hand_over(mixer_bufs, 6, *mixed_at(early_of(count))[:2])
    lane = lax.broadcasted_iota(jnp.int32, (half, LANES), 1)
    slot = lax.broadcasted_iota(jnp.int32, (half, LANES), 0)
    live = jnp.where(slot < lengths[0], 1.0, 0.0)
    loads[7].wait()
    for h in range(heads):
        old = state[h]
        top = old.astype(BF16)
        split[h, :, :HEAD_DIM] = top
        split[h, :, HEAD_DIM:] = (old - top.astype(F32)).astype(BF16)
    for stage, c in in_order(count)[:count]:
        rs_second(mixer_bufs, 6, c, *mixed_at(c))
    groups = [range(c, min(c + 2, count)) for c in range(0, count, 2)]
    scale, logits, grown = None, None, []
    for group_of in groups:
        for c in group_of:
            rs_wait(mixer_bufs, 6, c, *mixed_at(c))
        if scale is None:
            scale = inverse_rms(mixer_bufs)
            logits = total(mixer_bufs, LANES, LANES)
        for h in range(group_of[0] * batch, (group_of[-1] + 1) * batch):
            c = h // batch
            base = 2 * LANES + 2 * c * size + (h - c * batch) * HEAD_DIM
            both = total(mixer_bufs, base, HEAD_DIM)
            query, value = silu(both[:half] * scale), silu(both[half:] * scale)
            both = total(mixer_bufs, base + size, HEAD_DIM)
            keyvec, outgate = silu(both[:half] * scale), silu(both[half:] * scale)
            query = query * lax.rsqrt(jnp.sum(query * query, axis=1, keepdims=True) + EPS)
            query = query * HEAD_DIM ** (-0.5)
            keyvec = keyvec * lax.rsqrt(jnp.sum(keyvec * keyvec, axis=1, keepdims=True) + EPS)
            mine = lane == my_tp * heads + h
            beta_logit = jnp.sum(jnp.where(mine, logits[:half] * scale, 0.0), axis=1, keepdims=True)
            decay_logit = jnp.sum(jnp.where(mine, logits[half:] * scale, 0.0), axis=1, keepdims=True)
            beta_logit = jnp.broadcast_to(beta_logit, (half, LANES))
            decay_logit = jnp.broadcast_to(decay_logit, (half, LANES)) + decay_bias[0, h]
            beta = live / (1.0 + jnp.exp(-beta_logit))
            soft = jnp.maximum(decay_logit, 0.0) + jnp.log(1.0 + jnp.exp(-jnp.abs(decay_logit)))
            decay = -decay_rate[0, h] * soft * live
            reach = jnp.zeros_like(decay)
            for i in range(NEW):
                reach = reach + jnp.where(slot >= i, decay[i : i + 1], 0.0)
            before = jnp.exp(reach)
            asked = jnp.concatenate([keyvec, query], axis=0)
            top = asked.astype(BF16).astype(F32)
            found = jnp.dot(
                jnp.concatenate([top, asked - top], axis=0).astype(BF16),
                split[h],
                preferred_element_type=F32,
            )
            held = (
                found[: 2 * half, :HEAD_DIM]
                + found[2 * half :, :HEAD_DIM]
                + found[: 2 * half, HEAD_DIM:]
            )
            update = beta * (value - before * held[:half])
            output = before * held[half:]
            for i in range(NEW):
                between = jnp.where(slot >= i, jnp.exp(jnp.minimum(reach - reach[i : i + 1], 0.0)), 0.0)
                row = keyvec[i : i + 1]
                alike = jnp.sum(keyvec * row, axis=1, keepdims=True)
                fixed = update[i : i + 1]
                update = update - jnp.where(slot > i, beta * between * alike * fixed, 0.0)
                output = output + between * jnp.sum(query * row, axis=1, keepdims=True) * fixed
            last = reach[NEW - 1 : NEW]
            grown.append((keyvec, update * jnp.exp(last - reach), jnp.exp(last)))
            output = output * live
            output = output * lax.rsqrt(jnp.mean(output * output, axis=1, keepdims=True) + EPS)
            output = output * head_gain[...] * outgate
            hidden_mixer[my_plane, my_depth, :, h * HEAD_DIM : (h + 1) * HEAD_DIM] = output.astype(
                BF16
            )
        part = (group_of[0], group_of[0] * size, len(group_of) * size)
        ag_depth(mixer_bufs, 6, *part)
        ag_direct(mixer_bufs, 6, *part)
    for h, (keyvec, gained, kept) in enumerate(grown):
        zero = jnp.zeros_like(keyvec)
        new_state[0, h] = state[h] * kept + lax.dot_general(
            jnp.concatenate([keyvec, zero], axis=0),
            jnp.concatenate([gained, zero], axis=0),
            (((0,), (0,)), ((), ())),
            precision=lax.Precision.HIGHEST,
            preferred_element_type=F32,
        )
    loads[8].wait()
    branch = jnp.zeros((rows, width), F32)
    for group_of in groups:
        start, wide = group_of[0] * size, len(group_of) * size
        ag_near(mixer_bufs, 6, group_of[0], start, wide)
        ag_wait(mixer_bufs, 6, group_of[0], start, wide)
        branch = branch + jnp.dot(
            stacked(hidden_mixer, start, wide),
            out_w[start : start + wide, :],
            preferred_element_type=F32,
        )
    pair_mixer[my_tp] = branch
    all_tp(pair_mixer.at[my_tp], pair_mixer.at[my_tp], 2, pair_mixer.at[0])
    branch = pair_mixer[0]
    for t in range(1, tps):
        branch = branch + pair_mixer[t]
    resid[...] = (resid[...] + branch).astype(BF16).astype(F32)

    feed_forward(
        smalls[9:10], gain_second, second_gate, second_up, second_down, loads[9:12],
        second_bufs, pair_second, 12, 3,
    )
    arrived[...] = lax.dot_general(
        natural[...], resid[...].astype(BF16), (((0,), (0,)), ((), ())), preferred_element_type=F32
    )
    layer_out[...] = arrived[own, :].astype(BF16)
    all_sent(first_bufs, 0)
    all_sent(mixer_bufs, 6)
    all_sent(second_bufs, 12)


def solution(mesh):
    n, tps = mesh.shape["kv"], mesh.shape["tp"]

    def on_device(
        tokens,
        lengths,
        memory_state,
        gain_first,
        first_gate,
        first_up,
        first_down,
        gain_mixer,
        query_weight,
        key_weight,
        value_weight,
        outgate_weight,
        beta_weight,
        decay_weight,
        decay_rate,
        decay_bias,
        head_gain,
        out_weight,
        gain_second,
        second_gate,
        second_up,
        second_down,
    ):
        rows = tokens.shape[0] * tps
        width = tokens.shape[1]
        units = first_gate.shape[1]
        span = query_weight.shape[1]
        group = pieces(n, 4)
        depth = n // group
        half_parts = pieces(units // LANES, 4)
        mixer_parts = pieces(memory_state.shape[1], 4)
        vmem = pl.BlockSpec(memory_space=pltpu.VMEM)
        hbm = pl.BlockSpec(memory_space=pltpu.HBM)

        def like(array):
            return pltpu.VMEM(array.shape, array.dtype)

        def owners(before, sizes):
            swapped = swaps(len(sizes))
            last = sizes[-1] if swapped else LANES
            columns = before + sum(sizes)
            kept = columns - (last if swapped else 0)
            return (
                pltpu.VMEM((group, depth, 2 * NEW, columns), BF16),
                pltpu.VMEM((group, depth, 2 * NEW, kept), BF16),
                pltpu.VMEM((depth, 2 * NEW, kept), BF16),
                pltpu.VMEM((depth, 2 * NEW, kept), BF16),
                pltpu.VMEM((depth, group, 2 * NEW, last), BF16),
                pltpu.VMEM((group, 2 * NEW, last), BF16),
                pltpu.VMEM((group, 2 * NEW, last), BF16),
            )

        def gathered(columns):
            return pltpu.VMEM((group, depth, NEW, columns), BF16)

        def pairs():
            return pltpu.VMEM((tps, rows, width), F32)

        parts = pl.pallas_call(
            functools.partial(layer_kernel, n, tps),
            name="layer",
            out_shape=(
                pltpu.VMEM(tokens.shape, BF16),
                pltpu.VMEM(memory_state.shape, F32),
            ),
            in_specs=[hbm] * 22,
            out_specs=(vmem, vmem),
            scratch_shapes=[
                like(tokens),
                pltpu.SMEM(lengths.shape, lengths.dtype),
                pltpu.VMEM((1, width), F32),
                pltpu.VMEM((1, width), F32),
                pltpu.VMEM(beta_weight.shape[::-1], BF16),
                pltpu.VMEM(decay_weight.shape[::-1], BF16),
                pltpu.SMEM((1, decay_rate.shape[0]), F32),
                pltpu.SMEM((1, decay_bias.shape[0]), F32),
                pltpu.VMEM((1, HEAD_DIM), F32),
                pltpu.VMEM((1, width), F32),
                like(first_gate),
                like(first_up),
                like(first_down),
                like(query_weight),
                like(key_weight),
                like(value_weight),
                like(outgate_weight),
                like(out_weight),
                like(second_gate),
                like(second_up),
                like(second_down),
                pltpu.VMEM(memory_state.shape[1:], F32),
                pltpu.VMEM((*memory_state.shape[1:3], 2 * HEAD_DIM), BF16),
                pltpu.VMEM((rows, width), F32),
                pltpu.VMEM((2 * rows, rows), BF16),
                pltpu.VMEM((2 * rows, rows), BF16),
                pltpu.VMEM((rows, width), F32),
                pltpu.VMEM((rows, rows), BF16),
                owners(LANES, shares(units, half_parts)),
                owners(2 * LANES, [2 * span // mixer_parts] * mixer_parts),
                owners(LANES, shares(units, half_parts)),
                gathered(units),
                gathered(span),
                gathered(units),
                pairs(),
                pairs(),
                pairs(),
                pltpu.SemaphoreType.DMA((12,)),
                pltpu.SemaphoreType.DMA((18,)),
                pltpu.SemaphoreType.DMA((18, 4)),
                pltpu.SemaphoreType.DMA((2, 4)),
                pltpu.SemaphoreType.DMA((3,)),
                pltpu.SemaphoreType.REGULAR((3,)),
                pltpu.SemaphoreType.DMA((10,)),
            ],
            compiler_params=pltpu.CompilerParams(
                collective_id=0,
                has_side_effects=True,
                vmem_limit_bytes=60 * 1024 * 1024,
            ),
        )(
            tokens,
            lengths,
            memory_state,
            gain_first.reshape(1, -1),
            first_gate,
            first_up,
            first_down,
            gain_mixer.reshape(1, -1),
            query_weight,
            key_weight,
            value_weight,
            outgate_weight,
            beta_weight.T,
            decay_weight.T,
            decay_rate.reshape(1, -1),
            decay_bias.reshape(1, -1),
            head_gain.reshape(1, -1),
            out_weight,
            gain_second.reshape(1, -1),
            second_gate,
            second_up,
            second_down,
        )
        return pl.pallas_call(
            put_out,
            name="put_out",
            out_shape=(
                jax.ShapeDtypeStruct(tokens.shape, BF16),
                jax.ShapeDtypeStruct(memory_state.shape, F32),
            ),
            in_specs=[vmem, vmem],
            out_specs=(hbm, hbm),
            scratch_shapes=[pltpu.SemaphoreType.DMA((2,))],
            compiler_params=pltpu.CompilerParams(vmem_limit_bytes=2 * 1024 * 1024),
        )(*parts)

    in_specs = (
        P("tp", "kv"),
        P("kv"),
        P("kv", "tp", None, None),
        P("kv"),
        P("kv", "tp"),
        P("kv", "tp"),
        P("tp", "kv"),
        P("kv"),
        P("kv", "tp"),
        P("kv", "tp"),
        P("kv", "tp"),
        P("kv", "tp"),
        P("kv", None),
        P("kv", None),
        P("tp"),
        P("tp"),
        P(),
        P("tp", "kv"),
        P("kv"),
        P("kv", "tp"),
        P("kv", "tp"),
        P("tp", "kv"),
    )
    out_specs = (P("tp", "kv"), P("kv", "tp", None, None))
    return jax.shard_map(
        on_device, mesh=mesh, in_specs=in_specs, out_specs=out_specs, check_vma=False
    )
```
